32 devices in a mesh: fs: 8 (over z, x), tp: 4 (over y, core).
Axes of the slice: x: 2, y: 2, z: 4, core: 2. Of those that a mesh axis runs over, the one named last changes fastest.
Arguments:
- tokens: bfloat16 [2048, 2048], P('fs'), may hold values from -6 to 6
- norm_gain: float32 [2048], P('fs'), may hold values from 0.1 to 1.9
- gate_weight: float32 [8, 2048, 2048], P(None, 'fs', 'tp'), as said below
- up_weight: float32 [8, 2048, 2048], P(None, 'fs', 'tp'), as said below
- down_weight: float32 [8, 2048, 2048], P(None, 'fs', 'tp'), may hold values from -0.125 to 0.125
- routes: int32 [2048, 4], P('fs'), may hold values from 0 to 7, all different within a row; in each aligned block of 256 rows (0 to 255, 256 to 511, ...) at most 192 rows name the same one
- route_weights: bfloat16 [2048, 4], P('fs'), may hold values from 0.049804688 to 0.59765625
Outputs:
- gate_ready: bfloat16 [8, 2048, 2048], P('fs', None, 'tp')
- up_ready: bfloat16 [8, 2048, 2048], P('fs', None, 'tp')
- down_ready: bfloat16 [8, 2048, 2048], P('fs', None, 'tp')
- moe_output: bfloat16 [2048, 2048], P('fs', 'tp')
The draws below stay inside these ranges and needn't reach their ends.
Inputs may be any that keep to these rules, and one draw needn't show every extreme that they name: `routes`: each row names 4 different experts; among the rows of one index of fs no expert is named more than 192 times. `gate_weight`: real-valued entries, drawn afresh for each expert; the scale may differ from column to column. `up_weight`: real-valued entries, drawn afresh for each expert; the scale may differ from column to column.
All inputs are finite; a program needn't handle non-finite values.
Results may differ from the reference program's by a relative error of at most 0.015.
Values may be sent and summed in bfloat16 or wider, within the bound.
A program may use at most 128 MiB of HBM per device.

```python
import math
import jax
import jax.numpy as jnp
import numpy as np
from jax import lax

D = 2048
FF = 2048
TOP_K = 4
TOK_DEV = 256
EXPERTS = 8
CAP = 192
TOKENS = 2048
N_FS = 8
N_TP = 4


def clamped_weight(key, salt_value):
    inner_key = jax.random.fold_in(key, salt_value)
    drawn = jnp.clip(jax.random.normal(jax.random.fold_in(inner_key, 1), (EXPERTS, D, FF), jnp.float32), -6.0, 6.0) * D ** (-0.5)
    return drawn


def draw_gate_weight(key, part):
    return clamped_weight(key, 11)


def draw_up_weight(key, part):
    return clamped_weight(key, 23)


def block_levels(rng, extent, cuts, least, high):
    level = 1.0
    for axis_at, blocks in cuts:
        steps = jax.random.uniform(jax.random.fold_in(jax.random.fold_in(rng, 6), axis_at), (blocks,), jnp.float32, least / len(cuts), high / len(cuts))
        level = level * jnp.repeat(jnp.exp(steps), extent[axis_at] // blocks).reshape((-1,) + (1,) * (len(extent) - 1 - axis_at))
    return level


def shared_out(rng, own, number, rows, count, top, reach, lean):
    ranking = jax.random.permutation(rng, count)
    crowded, common = load_shares(count, rows * top, reach, lean, True), load_shares(count, rows * top, reach, lean, False)
    places = jnp.arange(count)

    def named(tallies, turn):
        used = int((tallies > 0).sum())
        fixed = max(1, used // 4)
        moved = fixed + (places - fixed + turn * (used - fixed)) % max(1, count - fixed)
        return jnp.zeros((count,), jnp.int32).at[ranking[jnp.where(places < fixed, places, moved)]].set(jnp.asarray(tallies, jnp.int32))

    tallies = jnp.where(number % 4 == 0, named(crowded, number // 4), named(common, number - number // 4 - 1))
    mixed = jax.random.permutation(jax.random.fold_in(own, 3), count)
    donor, receiver = mixed[0:count // 2 * 2:2], mixed[1:count // 2 * 2:2]
    slack = jnp.minimum(tallies[donor] - 1, reach - tallies[receiver]) // 2
    slack = jnp.where((donor == ranking[0]) | (receiver == ranking[0]) | (tallies[receiver] == 0), 0, jnp.maximum(slack, 0))
    moved = jax.random.randint(jax.random.fold_in(own, 4), (count // 2,), 0, 1 << 20) % (slack + 1)
    tallies = tallies.at[donor].add(-moved).at[receiver].add(moved)
    labels = jnp.searchsorted(jnp.cumsum(tallies), jnp.arange(rows * top), side="right").astype(jnp.int32)
    grid = labels.reshape(top, rows).T
    grid = grid[jax.random.permutation(jax.random.fold_in(own, 1), rows)]
    turn = jax.random.randint(jax.random.fold_in(own, 2), (rows, 1), 0, top)
    return jnp.take_along_axis(grid, (jnp.arange(top)[None, :] + turn) % top, axis=1)


def load_shares(amount, total, reach, skew, full):
    loads = [(1 << 20) // math.isqrt(rank ** skew) + 1 for rank in range(1, amount + 1)]
    largest = reach if full else min(reach, max(-(-total // amount), total * loads[0] // sum(loads)))
    least = 1 if total - largest >= amount - 1 else 0
    counts, rest = [largest] + [least] * (amount - 1), total - largest - least * (amount - 1)
    while rest > 0:
        movable = [i for i in range(1, amount) if counts[i] < largest] or [i for i in range(1, amount) if counts[i] < reach]
        mass, remaining = sum([loads[i] for i in movable]), rest
        for i in movable:
            extra = min(reach - counts[i], max(1, remaining * loads[i] // mass), rest)
            counts[i] = counts[i] + extra
            rest = rest - extra
    return np.array(counts)


def normal_values(own_key, shape, scale, bound, cuts=(), kind=jnp.bfloat16):
    result = scale * jax.random.normal(own_key, shape, jnp.float32)
    if cuts:
        result = result * block_levels(own_key, shape, cuts, -0.22, 0.18)
    return jnp.clip(result, -bound, bound).astype(kind)


def setup_inputs(seed: int = 0) -> dict:
    splits = jax.random.split(jax.random.key(seed), 8)
    tokens = normal_values(splits[0], (TOKENS, D), 1.0, 6.0, ((0, 8),))
    norm_gain = jnp.clip(1.0 + 0.18 * jax.random.normal(splits[1], (D,), jnp.float32), 0.1, 1.9)
    gate_weight = draw_gate_weight(jax.random.fold_in(splits[7], 71), 0)
    up_weight = draw_up_weight(jax.random.fold_in(splits[7], 71), 0)
    down_weight = normal_values(splits[4], (EXPERTS, D, FF), FF ** -0.5, 0.125, ((1, 8), (2, 4)), jnp.float32)
    routes_keys = jax.random.split(jax.random.fold_in(splits[5], 1), TOKENS // TOK_DEV)
    routes_turns = jax.random.permutation(jax.random.fold_in(splits[5], 3), TOKENS // TOK_DEV)
    routes = jax.vmap(lambda own, number: shared_out(jax.random.fold_in(splits[5], 2), own, number, TOK_DEV, EXPERTS, TOP_K, CAP, 2))(routes_keys, routes_turns).reshape((TOKENS, TOP_K))
    route_weights = jnp.clip(0.049804688 + 0.54785156 * jax.random.uniform(splits[6], (TOKENS, TOP_K), jnp.float32) ** block_levels(splits[6], (TOKENS, TOP_K), ((0, 8),), -0.2, 0.2), 0.049804688, 0.59765625).astype(jnp.bfloat16)
    return dict(tokens=tokens, norm_gain=norm_gain, gate_weight=gate_weight, up_weight=up_weight, down_weight=down_weight, routes=routes, route_weights=route_weights)


norm_eps = 1e-06
clamp_limit = 7.0
gate_alpha = 1.702

def slot_numbers(route_block, capacity, experts):
    flat_routes = route_block.reshape(-1)
    onehot = (flat_routes[:, None] == jnp.arange(experts, dtype=jnp.int32)[None, :]).astype(jnp.int32)
    earlier = jnp.cumsum(onehot, axis=0) - onehot
    position = lax.optimization_barrier(jnp.sum(earlier * onehot, axis=1))
    return (flat_routes * capacity + position).astype(jnp.int32)

def slot_sources(slots, top_count, tok_rows, total_slots):
    owners = (jnp.arange(slots.shape[0], dtype=jnp.int32) // top_count).astype(jnp.int32)
    return jnp.full((total_slots,), tok_rows, jnp.int32).at[slots].set(owners)

def combine_table(slots, weights_block, total_slots):
    matches = slots.reshape(weights_block.shape)[:, :, None] == jnp.arange(total_slots, dtype=jnp.int32)[None, None, :]
    table = lax.optimization_barrier(jnp.sum(jnp.where(matches, weights_block.astype(jnp.float32)[:, :, None], jnp.float32(0.0)), axis=1))
    return table.astype(jnp.bfloat16)

def activate(gate_pre, up_pre):
    gate_part = jnp.minimum(gate_pre, clamp_limit)
    up_part = jnp.clip(up_pre, -clamp_limit, clamp_limit)
    return (up_part + 1.0) * gate_part * jax.nn.sigmoid(gate_alpha * gate_part)

def reference(tokens, norm_gain, gate_weight, up_weight, down_weight, routes, route_weights):
    gain_col = norm_gain.astype(jnp.float32)[None, :, None]
    gate_ready = (gain_col * gate_weight).astype(jnp.bfloat16)
    up_ready = (gain_col * up_weight).astype(jnp.bfloat16)
    down_ready = down_weight.astype(jnp.bfloat16)
    wide_tokens = tokens.astype(jnp.float32)
    normed = (wide_tokens * lax.rsqrt(lax.optimization_barrier(jnp.mean(wide_tokens * wide_tokens, axis=1, keepdims=True)) + norm_eps)).astype(jnp.bfloat16)
    total_slots = EXPERTS * CAP
    route_blocks = routes.reshape(N_FS, TOK_DEV, TOP_K)
    slots = jax.vmap(lambda blk: slot_numbers(blk, CAP, EXPERTS))(route_blocks)
    sources = jax.vmap(lambda sl: slot_sources(sl, TOP_K, TOK_DEV, total_slots))(slots)
    padded = jnp.concatenate([normed.reshape(N_FS, TOK_DEV, D), jnp.zeros((N_FS, 1, D), jnp.bfloat16)], axis=1)
    dispatched = jax.vmap(lambda rows_blk, src: rows_blk[src])(padded, sources)
    per_expert = dispatched.reshape(N_FS, EXPERTS, CAP, D).transpose(1, 0, 2, 3).reshape(EXPERTS, N_FS * CAP, D)
    share = FF // N_TP

    def run_expert(operands):
        rows_in, gate_mat, up_mat, down_mat = operands
        gate_pre = jnp.dot(rows_in, gate_mat, preferred_element_type=jnp.float32)
        up_pre = jnp.dot(rows_in, up_mat, preferred_element_type=jnp.float32)
        hidden = activate(gate_pre, up_pre).astype(jnp.bfloat16)
        total = jnp.zeros((rows_in.shape[0], D), jnp.float32)
        for block_index in range(N_TP):
            hid_block = hidden[:, block_index * share:(block_index + 1) * share]
            down_block = down_mat[:, block_index * share:(block_index + 1) * share]
            partial_sum = lax.dot_general(hid_block, down_block, (((1,), (1,)), ((), ())), preferred_element_type=jnp.float32).astype(jnp.bfloat16)
            total = total + lax.optimization_barrier(partial_sum).astype(jnp.float32)
        return total.astype(jnp.bfloat16)
    expert_out = lax.map(run_expert, (per_expert, gate_ready, up_ready, down_ready))
    by_block = expert_out.reshape(EXPERTS, N_FS, CAP, D).transpose(1, 0, 2, 3).reshape(N_FS, total_slots, D)
    tables = jax.vmap(lambda sl, wb: combine_table(sl, wb, total_slots))(slots, route_weights.reshape(N_FS, TOK_DEV, TOP_K))
    mixed_rows = jnp.einsum('btj,bjd->btd', tables.astype(jnp.float32), by_block.astype(jnp.float32))
    moe_output = mixed_rows.reshape(N_FS * TOK_DEV, D).astype(jnp.bfloat16)
    return (gate_ready, up_ready, down_ready, moe_output)
```

```python
import functools

import jax
import jax.numpy as jnp
from jax import lax
from jax.experimental import pallas as pl
from jax.experimental.pallas import tpu as pltpu
from jax.sharding import PartitionSpec as P

norm_eps = 1e-06
clamp_limit = 7.0
gate_alpha = 1.702
MESH = pl.DeviceIdType.MESH
CORES = 2
DEPTH = 6
LANES = 128


def activate(gate_pre, up_pre):
    gate_part = jnp.minimum(gate_pre, clamp_limit)
    up_part = jnp.clip(up_pre, -clamp_limit, clamp_limit)
    return (up_part + 1.0) * gate_part * jax.nn.sigmoid(gate_alpha * gate_part)


def line_width(n):
    width = 1
    while 4 * width * width <= n:
        width *= 2
    return width


def kernel(
    n,
    groups,
    nx,
    row_tile,
    tokens,
    gain,
    routes,
    route_weights,
    gate_local,
    up_local,
    down_local,
    gate_ready,
    up_ready,
    down_ready,
    out,
    wide,
    token_rows,
    staged,
    gathered,
    meta,
    metas,
    tables,
    routed,
    gate_pre,
    hidden,
    given,
    kept,
    partner_sums,
    chip_sums,
    expert_out,
    row_sums,
    x_out,
    x_in,
    near_out,
    near_in,
    far_out,
    far_in,
    cross_out,
    cross_in,
    finished,
    wide_sem,
    token_sem,
    meta_send,
    meta_recv,
    token_send,
    token_recv,
    share_send,
    share_recv,
    forward_send,
    forward_recv,
    weight_send,
    weight_recv,
    down_send,
    down_recv,
    pair_send,
    pair_recv,
    chip_send,
    chip_recv,
    x_send,
    x_recv,
    near_send,
    near_recv,
    far_send,
    far_recv,
    cross_send,
    cross_recv,
):
    me = lax.axis_index("fs")
    tp = lax.axis_index("tp")
    chips = groups // CORES
    chip = tp // CORES
    core = lax.rem(tp, CORES)
    partner = chip * CORES + (CORES - 1 - core)
    nz = n // nx
    span = nz // 2
    z = me // nx
    x = lax.rem(me, nx)
    half = z // span
    local = lax.rem(z, span)
    gate_way = span - 1 + half
    far_way = span - half
    tok_rows, width = token_rows.shape
    part = width // groups
    source_rows = gate_local.shape[1]
    shares = n // groups
    total_slots = hidden.shape[0]
    capacity = total_slots // n
    chunks = given.shape[0]
    piece = source_rows // chunks
    f32, bf16 = jnp.float32, jnp.bfloat16

    def at(zz, xx):
        return zz * nx + xx

    def near(i):
        return half * span + lax.rem(local + i, span)

    def far(i):
        return (1 - half) * span + lax.rem(local + i, span)

    def beside(dx):
        return lax.rem(x + dx, nx)

    def slots_of(block):
        return pl.ds(pl.multiple_of(block * capacity, 16), capacity)

    def rows_of(block):
        return pl.ds(pl.multiple_of(block * source_rows, 16), source_rows)

    def chunk_of(block, i):
        return pl.ds(pl.multiple_of(block * source_rows + i * piece, 16), piece)

    sends = []

    def remote(src, dst, send_sem, recv_sem, device):
        return pltpu.make_async_remote_copy(
            src_ref=src,
            dst_ref=dst,
            send_sem=send_sem,
            recv_sem=recv_sem,
            device_id=device,
            device_id_type=MESH,
        )

    def push(src, dst, send_sem, recv_sem, device, keep=True):
        copy = remote(src, dst, send_sem, recv_sem, device)
        copy.start()
        if keep:
            sends.append(copy)
        return copy

    peers = [at(far(i), beside(dx)) for i in range(span) for dx in range(nx)]
    peers += [at(near(i), beside(dx)) for i in range(span) for dx in range(nx) if i + dx > 0]
    places = peers + [me]
    locals_ = (gate_local, up_local, down_local)
    readies = (gate_ready, up_ready, down_ready)
    blocks = [(j, q) for j in range(3) for q in range(n)]

    def fetch(i):
        j, q = blocks[i]
        copy = pltpu.make_async_copy(
            locals_[j].at[places[q]], wide.at[i % DEPTH], wide_sem.at[i % DEPTH]
        )
        copy.start()
        return copy

    token_copy = pltpu.make_async_copy(tokens, token_rows, token_sem)
    token_copy.start()
    fetches = [fetch(i) for i in range(DEPTH)]

    barrier = pltpu.get_barrier_semaphore()
    for k in range(1, n):
        pl.semaphore_signal(
            barrier, inc=1, device_id=(lax.rem(me + k, n), tp), device_id_type=MESH
        )
    for k in range(1, groups):
        pl.semaphore_signal(
            barrier, inc=1, device_id=(me, lax.rem(tp + k, groups)), device_id_type=MESH
        )

    token_copy.wait()

    @pl.loop(0, tok_rows // 32)
    def _(tile):
        rows = pl.ds(pl.multiple_of(tile * 32, 32), 32)
        wide_rows = token_rows[rows, :].astype(f32)
        scale = lax.rsqrt(jnp.mean(wide_rows * wide_rows, axis=1, keepdims=True) + norm_eps)
        columns = pl.ds(pl.multiple_of(tp * part, LANES), part)
        gathered[me, rows, :] = (token_rows[rows, columns].astype(f32) * scale).astype(bf16)

    ids = lax.broadcasted_iota(jnp.int32, (n, tok_rows), 0)
    member = jnp.zeros((n, tok_rows), f32)
    row_weight = jnp.zeros((n, tok_rows), f32)
    for k in range(routes.shape[0]):
        hit = routes[k : k + 1, :] == ids
        member += jnp.where(hit, 1.0, 0.0)
        row_weight += jnp.where(hit, route_weights[k : k + 1, :], 0.0)
    before = lax.broadcasted_iota(jnp.int32, (tok_rows, tok_rows), 0) < lax.broadcasted_iota(
        jnp.int32, (tok_rows, tok_rows), 1
    )
    counts = jnp.dot(member.astype(bf16), before.astype(bf16), preferred_element_type=f32)
    position = jnp.where(member > 0.0, counts, -1.0)
    meta[...] = jnp.zeros(meta.shape, f32)
    for e in range(n):
        meta[e, 0:1, :] = position[e : e + 1, :]
        meta[e, 1:2, :] = row_weight[e : e + 1, :]
    metas[me] = meta[me]

    pl.semaphore_wait(barrier, n + groups - 2)

    meta_copies = []
    for k in range(1, n):
        peer = lax.rem(me + k, n)
        meta_copies.append(
            push(meta.at[peer], metas.at[me], meta_send.at[k], meta_recv.at[k], (peer, tp))
        )

    spots = iter(range(token_send.shape[0]))

    def push_tokens(block, device_z, device_x, keep=True):
        spot = next(spots)
        return push(
            gathered.at[block],
            gathered.at[block],
            token_send.at[spot],
            token_recv.at[block],
            (at(device_z, device_x), tp),
            keep,
        )

    push_tokens(me, far_way, x)
    for i in range(1, span):
        push_tokens(me, near(i), x)
    for dx in range(1, nx):
        push_tokens(me, z, beside(dx))

    def push_weights(j, q):
        push(
            staged.at[j, q],
            readies[j].at[rows_of(me)],
            weight_send.at[j, q],
            weight_recv.at[j, me],
            (places[q], tp),
        )

    def convert(i):
        j, q = blocks[i]
        fetches[i].wait()
        value = wide[i % DEPTH]
        if j < 2:
            value = gain[...] * value
        if q == n - 1:
            readies[j][rows_of(me), :] = value.astype(bf16)
        else:
            staged[j, q] = value.astype(bf16)
        if i + DEPTH < len(blocks):
            fetches.append(fetch(i + DEPTH))

    for q in range(n):
        convert(q)
        if q > 0:
            push_weights(0, q - 1)
    for q in range(n):
        convert(n + q)

    for copy in meta_copies:
        copy.wait_recv()

    def await_tokens(block):
        remote(
            gathered.at[block],
            gathered.at[block],
            token_send.at[0],
            token_recv.at[block],
            (me, partner),
        ).wait_recv()

    def share_block(block):
        def to(step, device):
            remote(
                routed.at[tp, slots_of(block)],
                routed.at[tp, slots_of(block)],
                share_send.at[step],
                share_recv.at[step],
                (me, device),
            ).start()

        for h in range(1, chips):
            to(h, lax.rem(chip + h, chips) * CORES + core)
        to(0, partner)

    lines = lax.broadcasted_iota(jnp.int32, (capacity, tok_rows), 0).astype(f32)
    columns_of = lax.broadcasted_iota(jnp.int32, (tok_rows, capacity), 1).astype(f32)
    diagonal = lax.broadcasted_iota(jnp.int32, (tok_rows, tok_rows), 0) == lax.broadcasted_iota(
        jnp.int32, (tok_rows, tok_rows), 1
    )
    pending = []

    def pick(block):
        place = metas[block, 0:1, :]
        weight = metas[block, 1:2, :]
        chosen = jnp.where(place == lines, 1.0, 0.0).astype(bf16)
        routed[tp, slots_of(block), :] = jnp.dot(
            chosen, gathered[block], preferred_element_type=f32
        ).astype(bf16)
        if pending:
            share_block(pending.pop())
        ones = jnp.ones((tok_rows, capacity), bf16)
        place_down = jnp.dot(
            jnp.where(diagonal, place, 0.0).astype(bf16), ones, preferred_element_type=f32
        )
        weight_down = jnp.dot(
            jnp.where(diagonal, weight, 0.0).astype(bf16), ones, preferred_element_type=f32
        )
        tables[block] = jnp.where(place_down == columns_of, weight_down, 0.0).astype(bf16)
        pending.append(block)

    relays = []
    column = [near(i) for i in range(span)] + [far(i) for i in range(span)]
    for i in range(nz + 1):
        if i < nz:
            block = at(column[i], x)
            if i > 0:
                await_tokens(block)
                if i >= span:
                    spot = [next(spots) for _ in range(1, span)]

                    @pl.when(z == gate_way)
                    def _(block=block, spot=spot):
                        for m in range(1, span):
                            remote(
                                gathered.at[block],
                                gathered.at[block],
                                token_send.at[spot[m - 1]],
                                token_recv.at[block],
                                (at(near(m), x), tp),
                            ).start()

                    relays += [(block, spot[m - 1], near(m)) for m in range(1, span)]
                for dx in range(1, nx):
                    push_tokens(block, z, beside(dx))
        if i > 0:
            for dx in range(1, nx):
                other = at(column[i - 1], beside(dx))
                await_tokens(other)
                pick(other)
        if i < nz:
            pick(block)
    share_block(pending.pop())

    for q in range(n - 1):
        push_weights(1, q)
    for q in range(n):
        convert(2 * n + q)

    def all_rows(step, origin, device):
        return remote(
            routed.at[tp], routed.at[origin], share_send.at[step], share_recv.at[step], (me, device)
        )

    shared = []
    for h in range(1, chips):
        origin = lax.rem(chip - h + chips, chips) * CORES + core
        copy = all_rows(h, origin, partner)
        copy.wait_recv()
        shared.append(copy)
        push(
            routed.at[origin],
            routed.at[origin],
            forward_send.at[h],
            forward_recv.at[h],
            (me, partner),
        )
    copy = all_rows(0, partner, partner)
    copy.wait_recv()
    shared.append(copy)
    for h in range(1, chips):
        origin = lax.rem(chip - h + chips, chips) * CORES + (CORES - 1 - core)
        remote(
            routed.at[origin],
            routed.at[origin],
            forward_send.at[h],
            forward_recv.at[h],
            (me, partner),
        ).wait_recv()

    def await_weights(j):
        for k in range(1, n):
            source = lax.rem(me + k, n)
            remote(
                staged.at[j, 0],
                readies[j].at[rows_of(source)],
                weight_send.at[j, 0],
                weight_recv.at[j, source],
                (me, partner),
            ).wait_recv()

    def product(rows, ready):
        total = jnp.zeros((row_tile, hidden.shape[1]), f32)
        for t in range(groups):
            total += jnp.dot(
                routed[t, rows, :],
                ready[t * part : (t + 1) * part],
                preferred_element_type=f32,
            )
        return total

    def tiles(body):
        @pl.loop(0, total_slots // row_tile)
        def _(tile):
            body(pl.ds(pl.multiple_of(tile * row_tile, 16), row_tile))

    await_weights(0)

    @tiles
    def _(rows):
        gate_pre[rows, :] = product(rows, gate_ready)

    def push_down(i):
        for q in range(n - 1):
            push(
                staged.at[2, q, pl.ds(i * piece, piece)],
                down_ready.at[chunk_of(me, i)],
                down_send.at[i, q],
                down_recv.at[i, me],
                (places[q], tp),
            )

    for i in range(min(2, chunks)):
        push_down(i)

    await_weights(1)

    @tiles
    def _(rows):
        hidden[rows, :] = activate(gate_pre[rows, :], product(rows, up_ready)).astype(bf16)

    over_copies = {}

    def project(i):
        for k in range(1, n):
            source = lax.rem(me + k, n)
            remote(
                staged.at[2, 0, pl.ds(0, piece)],
                down_ready.at[chunk_of(source, i)],
                down_send.at[i, 0],
                down_recv.at[i, source],
                (me, partner),
            ).wait_recv()

        def run(side, target):
            picked = [
                down_ready[
                    chunk_of((lax.rem(chip + h, chips) * CORES + side) * shares + r, i), :
                ]
                for h in range(chips)
                for r in range(shares)
            ]
            down = jnp.concatenate(picked, axis=0)

            @tiles
            def _(rows):
                value = lax.dot_general(
                    hidden[rows, :], down, (((1,), (1,)), ((), ())), preferred_element_type=f32
                ).astype(bf16)
                for h in range(chips):
                    target[i, h, rows, :] = value[:, h * LANES : (h + 1) * LANES]

        run(CORES - 1 - core, given)
        pair = push(
            given.at[i], partner_sums.at[i], pair_send.at[i], pair_recv.at[i], (me, partner)
        )
        run(core, kept)
        pair.wait_recv()
        for h in range(1, chips):

            @tiles
            def _(rows, h=h):
                total = kept[i, h, rows, :].astype(f32) + partner_sums[i, h, rows, :].astype(f32)
                kept[i, h, rows, :] = total.astype(bf16)

            over_copies[i, h] = push(
                kept.at[i, h],
                chip_sums.at[i, h - 1],
                chip_send.at[i, h],
                chip_recv.at[i, h],
                (me, lax.rem(chip + h, chips) * CORES + core),
            )

    x_copies = {}

    def combine(i):
        for h in range(1, chips):
            over_copies[i, h].wait_recv()

        @tiles
        def _(rows):
            total = kept[i, 0, rows, :].astype(f32) + partner_sums[i, 0, rows, :].astype(f32)
            for h in range(1, chips):
                total += chip_sums[i, h - 1, rows, :].astype(f32)
            expert_out[rows, :] = total.astype(bf16)

        def rows_for(block):
            return jnp.dot(
                tables[block], expert_out[slots_of(block), :], preferred_element_type=f32
            )

        for dx in range(1, nx):
            for zz in range(nz):
                x_out[i, dx - 1, zz] = rows_for(at(zz, beside(dx))).astype(bf16)
            x_copies[i, dx] = push(
                x_out.at[i, dx - 1],
                x_in.at[i, dx - 1],
                x_send.at[i, dx],
                x_recv.at[i, dx],
                (at(z, beside(dx)), tp),
            )
        for zz in range(nz):
            row_sums[i, zz] = rows_for(at(zz, x))

    near_copies = {}

    def far_copy(i, device_z, slot):
        return remote(
            far_out.at[i],
            far_in.at[i, slot],
            far_send.at[i],
            far_recv.at[i, slot],
            (at(device_z, x), tp),
        )

    def spread(i):
        for dx in range(1, nx):
            x_copies[i, dx].wait_recv()
        for zz in range(nz):
            total = row_sums[i, zz]
            for dx in range(1, nx):
                total += x_in[i, dx - 1, zz].astype(f32)
            row_sums[i, zz] = total

        @pl.when(z != gate_way)
        def _():
            for f in range(span):
                far_out[i, f] = row_sums[i, (1 - half) * span + f].astype(bf16)
            far_copy(i, gate_way, local).start()

        for m in range(1, span):
            near_out[i, m - 1] = row_sums[i, near(m)].astype(bf16)
            near_copies[i, m] = push(
                near_out.at[i, m - 1],
                near_in.at[i, m - 1],
                near_send.at[i, m],
                near_recv.at[i, m],
                (at(near(m), x), tp),
            )

    def cross_copy(i, f):
        return remote(
            cross_out.at[i, f],
            cross_in.at[i],
            cross_send.at[i, f],
            cross_recv.at[i],
            (at((1 - half) * span + f, x), tp),
        )

    def cross(i):
        @pl.when(z == gate_way)
        def _():
            for m in range(1, span):
                far_copy(i, near(m), lax.rem(local + m, span)).wait_recv()
            for f in range(span):
                total = row_sums[i, (1 - half) * span + f]
                for m in range(1, span):
                    total += far_in[i, lax.rem(local + m, span), f].astype(f32)
                cross_out[i, f] = total.astype(bf16)
                cross_copy(i, f).start()

    def finish(i):
        total = row_sums[i, z]
        for m in range(1, span):
            near_copies[i, m].wait_recv()
            total += near_in[i, m - 1].astype(f32)
        cross_copy(i, 0).wait_recv()
        total += cross_in[i].astype(f32)
        finished[:, i * LANES : (i + 1) * LANES] = total.astype(bf16)

    stages = (finish, cross, spread, combine)
    for step in range(chunks + len(stages)):
        for late, stage in enumerate(stages):
            i = step - (len(stages) - late)
            if 0 <= i < chunks:
                stage(i)
        if step < chunks:
            if step + 2 < chunks:
                push_down(step + 2)
            project(step)

    column_to = lax.broadcasted_iota(jnp.int32, (part, part), 1)
    share_to = column_to // source_rows
    inner_to = lax.rem(column_to, source_rows)
    from_to = (inner_to // piece) * LANES + share_to * piece + lax.rem(inner_to, piece)
    order = (lax.broadcasted_iota(jnp.int32, (part, part), 0) == from_to).astype(bf16)
    out[...] = jnp.dot(finished[...], order, preferred_element_type=f32).astype(bf16)

    @pl.when(z == gate_way)
    def _():
        for block, spot, device_z in relays:
            remote(
                gathered.at[block],
                gathered.at[block],
                token_send.at[spot],
                token_recv.at[block],
                (at(device_z, x), tp),
            ).wait_send()
        for i in range(chunks):
            for f in range(span):
                cross_copy(i, f).wait_send()

    @pl.when(z != gate_way)
    def _():
        for i in range(chunks):
            far_copy(i, gate_way, local).wait_send()

    for copy in sends + shared:
        copy.wait_send()


def hand_over(tokens, gain, routes, route_weights, gate_local, up_local, down_local):
    n = lax.axis_size("fs")
    groups = lax.axis_size("tp")
    tok_rows, width = tokens.shape
    top_count = routes.shape[0]
    source_rows, units = gate_local.shape[1:]
    capacity = 3 * tok_rows * top_count // (2 * n)
    total_slots = n * capacity
    part = width // groups
    chips = groups // CORES
    nx = line_width(n)
    nz = n // nx
    span = nz // 2
    chunks = part // LANES
    vmem = pl.BlockSpec(memory_space=pltpu.VMEM)
    anywhere = pl.BlockSpec(memory_space=pl.ANY)
    bf16, f32 = jnp.bfloat16, jnp.float32
    ready = jax.ShapeDtypeStruct((width, units), bf16)
    dma = pltpu.SemaphoreType.DMA
    token_sends = 1 + (span - 1) + nz * (nx - 1) + span * (span - 1)
    rows = (tok_rows, LANES)
    return pl.pallas_call(
        functools.partial(kernel, n, groups, nx, total_slots // 4),
        out_shape=(ready, ready, ready, jax.ShapeDtypeStruct((tok_rows, part), bf16)),
        in_specs=[anywhere] + [vmem] * 3 + [anywhere] * 3,
        out_specs=(vmem,) * 4,
        scratch_shapes=[
            pltpu.VMEM((DEPTH, source_rows, units), f32),
            pltpu.VMEM((tok_rows, width), bf16),
            pltpu.VMEM((3, n - 1, source_rows, units), bf16),
            pltpu.VMEM((n, tok_rows, part), bf16),
            pltpu.VMEM((n, 8, tok_rows), f32),
            pltpu.VMEM((n, 8, tok_rows), f32),
            pltpu.VMEM((n, tok_rows, capacity), bf16),
            pltpu.VMEM((groups, total_slots, part), bf16),
            pltpu.VMEM((total_slots, units), f32),
            pltpu.VMEM((total_slots, units), bf16),
            pltpu.VMEM((chunks, chips, total_slots, LANES), bf16),
            pltpu.VMEM((chunks, chips, total_slots, LANES), bf16),
            pltpu.VMEM((chunks, chips, total_slots, LANES), bf16),
            pltpu.VMEM((chunks, chips - 1, total_slots, LANES), bf16),
            pltpu.VMEM((total_slots, LANES), bf16),
            pltpu.VMEM((chunks, nz) + rows, f32),
            pltpu.VMEM((chunks, nx - 1, nz) + rows, bf16),
            pltpu.VMEM((chunks, nx - 1, nz) + rows, bf16),
            pltpu.VMEM((chunks, span) + rows, bf16),
            pltpu.VMEM((chunks, span) + rows, bf16),
            pltpu.VMEM((chunks, span) + rows, bf16),
            pltpu.VMEM((chunks, span, span) + rows, bf16),
            pltpu.VMEM((chunks, span) + rows, bf16),
            pltpu.VMEM((chunks,) + rows, bf16),
            pltpu.VMEM((tok_rows, part), bf16),
            dma((DEPTH,)),
            dma,
            dma((n,)),
            dma((n,)),
            dma((token_sends,)),
            dma((n,)),
            dma((chips,)),
            dma((chips,)),
            dma((chips,)),
            dma((chips,)),
            dma((2, n)),
            dma((2, n)),
            dma((chunks, n)),
            dma((chunks, n)),
            dma((chunks,)),
            dma((chunks,)),
            dma((chunks, chips)),
            dma((chunks, chips)),
            dma((chunks, nx)),
            dma((chunks, nx)),
            dma((chunks, span)),
            dma((chunks, span)),
            dma((chunks,)),
            dma((chunks, span)),
            dma((chunks, span)),
            dma((chunks,)),
        ],
        compiler_params=pltpu.CompilerParams(
            collective_id=0, has_side_effects=True, vmem_limit_bytes=58 * 1024 * 1024
        ),
    )(tokens, gain, routes, route_weights, gate_local, up_local, down_local)


def body(tokens, norm_gain, gate_weight, up_weight, down_weight, routes, route_weights):
    gate_ready, up_ready, down_ready, moe_output = hand_over(
        tokens,
        norm_gain[:, None],
        routes.T,
        route_weights.T.astype(jnp.float32),
        gate_weight,
        up_weight,
        down_weight,
    )
    return (gate_ready[None], up_ready[None], down_ready[None], moe_output)


def solution(mesh):
    in_specs = (
        P("fs", None),
        P("fs"),
        P(None, "fs", "tp"),
        P(None, "fs", "tp"),
        P(None, "fs", "tp"),
        P("fs", None),
        P("fs", None),
    )
    out_specs = (P("fs", None, "tp"), P("fs", None, "tp"), P("fs", None, "tp"), P("fs", "tp"))
    return jax.shard_map(body, mesh=mesh, in_specs=in_specs, out_specs=out_specs, check_vma=False)
```

```python
import functools

import jax
import jax.numpy as jnp
from jax import lax
from jax.experimental import pallas as pl
from jax.experimental.pallas import tpu as pltpu
from jax.sharding import PartitionSpec as P

norm_eps = 1e-06
clamp_limit = 7.0
gate_alpha = 1.702
MESH = pl.DeviceIdType.MESH
CORES = 2
DEPTH = 6
LANES = 128


def activate(gate_pre, up_pre):
    gate_part = jnp.minimum(gate_pre, clamp_limit)
    up_part = jnp.clip(up_pre, -clamp_limit, clamp_limit)
    return (up_part + 1.0) * gate_part * jax.nn.sigmoid(gate_alpha * gate_part)


def line_width(n):
    width = 1
    while 4 * width * width <= n:
        width *= 2
    return width


def kernel(
    n,
    groups,
    nx,
    row_tile,
    tokens,
    gain_in,
    routes_in,
    route_weights_in,
    gate_local,
    up_local,
    down_local,
    gate_ready,
    up_ready,
    down_ready,
    out,
    wide,
    token_rows,
    gain_row,
    gain,
    scale,
    routes,
    route_weights,
    staged,
    gathered,
    meta,
    metas,
    tables,
    routed,
    gate_pre,
    hidden,
    given,
    kept,
    partner_sums,
    chip_sums,
    expert_out,
    row_sums,
    x_out,
    x_in,
    near_out,
    near_in,
    far_out,
    far_in,
    cross_out,
    cross_in,
    finished,
    wide_sem,
    input_sem,
    meta_send,
    meta_recv,
    token_send,
    relay_send,
    token_recv,
    share_send,
    share_recv,
    forward_send,
    forward_recv,
    weight_send,
    weight_recv,
    down_recv,
    pair_send,
    pair_recv,
    chip_send,
    chip_recv,
    x_send,
    x_recv,
    near_send,
    near_recv,
    far_send,
    far_recv,
    cross_send,
    cross_recv,
):
    me = lax.axis_index("fs")
    tp = lax.axis_index("tp")
    chips = groups // CORES
    chip = tp // CORES
    core = lax.rem(tp, CORES)
    partner = chip * CORES + (CORES - 1 - core)
    nz = n // nx
    span = nz // 2
    z = me // nx
    x = lax.rem(me, nx)
    half = z // span
    local = lax.rem(z, span)
    gate_way = span - 1 + half
    far_way = span - half
    tok_rows, width = token_rows.shape
    part = width // groups
    source_rows = gate_local.shape[1]
    shares = n // groups
    total_slots = hidden.shape[0]
    capacity = total_slots // n
    chunks = given.shape[0]
    piece = source_rows // chunks
    f32, bf16 = jnp.float32, jnp.bfloat16

    def at(zz, xx):
        return zz * nx + xx

    def near(i):
        return half * span + lax.rem(local + i, span)

    def far(i):
        return (1 - half) * span + lax.rem(local + i, span)

    def beside(dx):
        return lax.rem(x + dx, nx)

    def slots_of(block):
        return pl.ds(pl.multiple_of(block * capacity, 16), capacity)

    def rows_of(block):
        return pl.ds(pl.multiple_of(block * source_rows, 16), source_rows)

    def chunk_of(block, i):
        return pl.ds(pl.multiple_of(block * source_rows + i * piece, 16), piece)

    group_rows = nx * capacity
    lane_rows = tok_rows // LANES

    def remote(src, dst, send_sem, recv_sem, device):
        return pltpu.make_async_remote_copy(
            src_ref=src,
            dst_ref=dst,
            send_sem=send_sem,
            recv_sem=recv_sem,
            device_id=device,
            device_id_type=MESH,
        )

    def push(src, dst, send_sem, recv_sem, device):
        copy = remote(src, dst, send_sem, recv_sem, device)
        copy.start()
        return copy

    def bulk(ref, send_sem, recv_sem):
        return remote(ref, ref, send_sem, recv_sem, (me, partner))

    peers = [at(far(i), beside(dx)) for dx in range(nx) for i in range(span)]
    peers += [at(near(i), beside(dx)) for dx in range(nx) for i in range(span) if i + dx > 0]
    places = peers + [me]
    locals_ = (gate_local, up_local, down_local)
    readies = (gate_ready, up_ready, down_ready)
    blocks = [(j, q) for j in range(3) for q in range(n)]

    def fetch(i):
        j, q = blocks[i]
        copy = pltpu.make_async_copy(
            locals_[j].at[places[q]], wide.at[i % DEPTH], wide_sem.at[i % DEPTH]
        )
        copy.start()
        return copy

    inputs = [
        pltpu.make_async_copy(src, dst, input_sem.at[spot])
        for spot, (src, dst) in enumerate(
            (
                (gain_in, gain_row),
                (tokens, token_rows),
                (routes_in, routes),
                (route_weights_in, route_weights),
            )
        )
    ]
    own_columns = pl.ds(pl.multiple_of(tp * part, LANES), part)
    inputs.append(
        pltpu.make_async_copy(tokens.at[:, own_columns], gathered.at[me], input_sem.at[4])
    )
    for copy in inputs:
        copy.start()
    fetches = [fetch(i) for i in range(DEPTH)]

    barrier = pltpu.get_barrier_semaphore()
    for k in range(1, n):
        pl.semaphore_signal(
            barrier, inc=1, device_id=(lax.rem(me + k, n), tp), device_id_type=MESH
        )
    for k in range(1, groups):
        pl.semaphore_signal(
            barrier, inc=1, device_id=(me, lax.rem(tp + k, groups)), device_id_type=MESH
        )

    inputs[0].wait()
    gain_at = lax.broadcasted_iota(jnp.int32, (source_rows, source_rows), 0) == (
        lax.broadcasted_iota(jnp.int32, (source_rows, source_rows), 1)
    )
    gain[...] = jnp.sum(jnp.where(gain_at, gain_row[...], 0.0), axis=1, keepdims=True)

    def push_weights(j, q):
        push(
            staged.at[j, q],
            readies[j].at[rows_of(me)],
            weight_send,
            weight_recv.at[j],
            (places[q], tp),
        )

    def convert(i):
        j, q = blocks[i]
        fetches[i].wait()
        value = wide[i % DEPTH]
        if j < 2:
            value = gain[...] * value
        if q == n - 1:
            readies[j][rows_of(me), :] = value.astype(bf16)
        else:
            staged[j, q] = value.astype(bf16)
        if i + DEPTH < len(blocks):
            fetches.append(fetch(i + DEPTH))

    pl.semaphore_wait(barrier, n + groups - 2)

    def push_tokens(block, device_z, device_x):
        push(
            tokens.at[:, own_columns],
            gathered.at[block],
            token_send,
            token_recv.at[block],
            (at(device_z, device_x), tp),
        )

    beside_half = [(i, dx) for dx in range(nx) for i in range(span) if i + dx > 0]
    push_tokens(me, far_way, x)
    for i, dx in beside_half:
        push_tokens(me, near(i), beside(dx))
    convert(0)
    for copy in inputs[1:]:
        copy.wait()

    @pl.loop(0, tok_rows // 32)
    def _(tile):
        rows = pl.ds(pl.multiple_of(tile * 32, 32), 32)
        wide_rows = token_rows[rows, :].astype(f32)
        scale[rows, :] = lax.rsqrt(
            jnp.mean(wide_rows * wide_rows, axis=1, keepdims=True) + norm_eps
        )

    ids = lax.broadcasted_iota(jnp.int32, (n, tok_rows), 0)
    member = jnp.zeros((n, tok_rows), f32)
    row_weight = jnp.zeros((n, tok_rows), f32)
    given_weights = route_weights[...].astype(f32)
    for k in range(routes.shape[0]):
        hit = routes[k : k + 1, :] == ids
        member += jnp.where(hit, 1.0, 0.0)
        row_weight += jnp.where(hit, given_weights[k : k + 1, :], 0.0)
    down_index = lax.broadcasted_iota(jnp.int32, (tok_rows, tok_rows), 0)
    across_index = lax.broadcasted_iota(jnp.int32, (tok_rows, tok_rows), 1)
    before = down_index < across_index
    diagonal = down_index == across_index
    scale_row = jnp.sum(jnp.where(diagonal, scale[...], 0.0), axis=0, keepdims=True)
    counts = jnp.dot(member.astype(bf16), before.astype(bf16), preferred_element_type=f32)
    position = jnp.where(member > 0.0, counts, -1.0)
    meta[...] = jnp.zeros(meta.shape, f32)
    for e in range(n):
        for r in range(lane_rows):
            lanes = slice(r * LANES, (r + 1) * LANES)
            meta[e, r : r + 1, :] = position[e : e + 1, lanes]
            meta[e, lane_rows + r : lane_rows + r + 1, :] = row_weight[e : e + 1, lanes]
            meta[e, 2 * lane_rows + r : 2 * lane_rows + r + 1, :] = scale_row[:, lanes]
    metas[me] = meta[me]

    for k in range(1, n):
        peer = lax.rem(me + k, n)
        push(meta.at[peer], metas.at[me], meta_send, meta_recv, (peer, tp))

    for q in range(1, n):
        convert(q)
        if q <= span:
            push_weights(0, q - 1)
    for q in range(n):
        convert(n + q)

    def push_rest():
        for q in range(span, n - 1):
            push_weights(0, q)

    def push_up():
        for q in range(n - 1):
            push_weights(1, q)

    @pl.when(z != gate_way)
    def _():
        push_rest()
        push_up()

    bulk(metas.at[pl.ds(0, n - 1)], meta_send, meta_recv).wait_recv()

    def await_tokens(block):
        bulk(gathered.at[block], token_send, token_recv.at[block]).wait_recv()

    def share_block(block):
        def to(step, device):
            remote(
                routed.at[tp, slots_of(block)],
                routed.at[tp, slots_of(block)],
                share_send.at[step],
                share_recv.at[step],
                (me, device),
            ).start()

        for h in range(1, chips):
            to(h, lax.rem(chip + h, chips) * CORES + core)
        to(0, partner)

    lines = lax.broadcasted_iota(jnp.int32, (capacity, tok_rows), 0).astype(f32)
    columns_of = lax.broadcasted_iota(jnp.int32, (tok_rows, capacity), 1).astype(f32)
    pending = []

    def pick(block):
        found = metas[block]
        place, weight, scale_across = (
            jnp.concatenate([found[j + r : j + r + 1, :] for r in range(lane_rows)], axis=1)
            for j in (0, lane_rows, 2 * lane_rows)
        )
        chosen = jnp.where(place == lines, 1.0, 0.0).astype(bf16)
        scale_down = jnp.sum(jnp.where(diagonal, scale_across, 0.0), axis=1, keepdims=True)
        normed = (gathered[block].astype(f32) * scale_down).astype(bf16)
        routed[tp, slots_of(block), :] = jnp.dot(
            chosen, normed, preferred_element_type=f32
        ).astype(bf16)
        if pending:
            share_block(pending.pop())
        ones = jnp.ones((tok_rows, capacity), bf16)
        place_down = jnp.dot(
            jnp.where(diagonal, place, 0.0).astype(bf16), ones, preferred_element_type=f32
        )
        weight_down = jnp.dot(
            jnp.where(diagonal, weight, 0.0).astype(bf16), ones, preferred_element_type=f32
        )
        tables[block] = jnp.where(place_down == columns_of, weight_down, 0.0).astype(bf16)
        pending.append(block)

    pick(me)
    for i, dx in beside_half:
        block = at(near(i), beside(dx))
        await_tokens(block)
        pick(block)
    for i in range(span):
        block = at(far(i), x)
        await_tokens(block)

        @pl.when(z == gate_way)
        def _(i=i, block=block):
            for m, dx in beside_half:
                push(
                    gathered.at[block],
                    gathered.at[block],
                    relay_send.at[i],
                    token_recv.at[block],
                    (at(near(m), beside(dx)), tp),
                )

    pl.when(z == gate_way)(push_rest)
    for dx in range(nx):
        for i in range(span):
            block = at(far(i), beside(dx))
            if dx > 0:
                await_tokens(block)
            pick(block)
    share_block(pending.pop())

    pl.when(z == gate_way)(push_up)
    for q in range(n):
        convert(2 * n + q)

    def all_rows(step, origin, device):
        return remote(
            routed.at[tp], routed.at[origin], share_send.at[step], share_recv.at[step], (me, device)
        )

    shared = []
    for h in range(1, chips):
        origin = lax.rem(chip - h + chips, chips) * CORES + core
        copy = all_rows(h, origin, partner)
        copy.wait_recv()
        shared.append(copy)
        push(
            routed.at[origin],
            routed.at[origin],
            forward_send.at[h],
            forward_recv.at[h],
            (me, partner),
        )
    copy = all_rows(0, partner, partner)
    copy.wait_recv()
    shared.append(copy)
    for h in range(1, chips):
        origin = lax.rem(chip - h + chips, chips) * CORES + (CORES - 1 - core)
        remote(
            routed.at[origin],
            routed.at[origin],
            forward_send.at[h],
            forward_recv.at[h],
            (me, partner),
        ).wait_recv()

    def await_weights(j):
        received = readies[j].at[pl.ds(0, (n - 1) * source_rows)]
        bulk(received, weight_send, weight_recv.at[j]).wait_recv()

    def product(rows, ready):
        total = jnp.zeros((row_tile, hidden.shape[1]), f32)
        for t in range(groups):
            total += jnp.dot(
                routed[t, rows, :],
                ready[t * part : (t + 1) * part],
                preferred_element_type=f32,
            )
        return total

    def tiles(body):
        @pl.loop(0, total_slots // row_tile)
        def _(tile):
            body(pl.ds(pl.multiple_of(tile * row_tile, 16), row_tile))

    await_weights(0)

    @tiles
    def _(rows):
        gate_pre[rows, :] = product(rows, gate_ready)

    def push_down(i):
        for q in range(n - 1):
            push(
                staged.at[2, q, pl.ds(i * piece, piece)],
                down_ready.at[chunk_of(me, i)],
                weight_send,
                down_recv.at[i],
                (places[q], tp),
            )

    @pl.when(z == gate_way)
    def _():
        for i in range(chunks):
            push_down(i)

    await_weights(1)
    pl.when(z != gate_way)(functools.partial(push_down, 0))

    @tiles
    def _(rows):
        hidden[rows, :] = activate(gate_pre[rows, :], product(rows, up_ready)).astype(bf16)

    over_copies = {}
    units = [(1 - half) * span + f for f in range(span)]
    units += [near(m) for m in range(1, span)] + [z]
    mates = range(span, nz - 1)
    own_unit = nz - 1

    def rows_in(u):
        return pl.ds(pl.multiple_of(units[u] * group_rows, 16), group_rows)

    def project(i):
        received = down_ready.at[pl.ds(0, (n - 1) * piece)]
        bulk(received, weight_send, down_recv.at[i]).wait_recv()
        if i + 1 < chunks:
            pl.when(z != gate_way)(functools.partial(push_down, i + 1))

        def rows_to(side):
            picked = [
                down_ready[
                    chunk_of((lax.rem(chip + h, chips) * CORES + side) * shares + r, i), :
                ]
                for h in range(chips)
                for r in range(shares)
            ]
            return jnp.concatenate(picked, axis=0)

        def run(down, target, u):
            rows = rows_in(u)
            value = lax.dot_general(
                hidden[rows, :], down, (((1,), (1,)), ((), ())), preferred_element_type=f32
            ).astype(bf16)
            for h in range(chips):
                target[i, h, rows, :] = value[:, h * LANES : (h + 1) * LANES]

        give = rows_to(CORES - 1 - core)
        for u in range(nz):
            run(give, given, u)
            for h in range(chips):
                push(
                    given.at[i, h, rows_in(u)],
                    partner_sums.at[i, h, rows_in(u)],
                    pair_send,
                    pair_recv.at[i, u],
                    (me, partner),
                )
        keep = rows_to(core)
        for u in range(nz):
            rows = rows_in(u)
            run(keep, kept, u)
            bulk(given.at[i, pl.ds(0, chips), rows], pair_send, pair_recv.at[i, u]).wait_recv()
            for h in range(1, chips):
                total = kept[i, h, rows, :].astype(f32)
                total += partner_sums[i, h, rows, :].astype(f32)
                kept[i, h, rows, :] = total.astype(bf16)
                over_copies[i, h, u] = push(
                    kept.at[i, h, rows],
                    chip_sums.at[i, h - 1, rows],
                    chip_send,
                    chip_recv.at[i, h, u],
                    (me, lax.rem(chip + h, chips) * CORES + core),
                )

    x_copies = {}

    def combine(i, u):
        for h in range(1, chips):
            over_copies[i, h, u].wait_recv()

        rows = rows_in(u)
        total = kept[i, 0, rows, :].astype(f32) + partner_sums[i, 0, rows, :].astype(f32)
        for h in range(1, chips):
            total += chip_sums[i, h - 1, rows, :].astype(f32)
        expert_out[rows, :] = total.astype(bf16)

        def rows_for(xx):
            block = at(units[u], xx)
            return jnp.dot(
                tables[block], expert_out[slots_of(block), :], preferred_element_type=f32
            )

        for dx in range(1, nx):
            x_out[i, dx - 1, u] = rows_for(beside(dx)).astype(bf16)
            x_copies[i, dx, u] = push(
                x_out.at[i, dx - 1, u],
                x_in.at[i, dx - 1, u],
                x_send,
                x_recv.at[i, dx, u],
                (at(z, beside(dx)), tp),
            )
        row_sums[i, u] = rows_for(x)

    near_copies = {}

    def far_copy(i, u, device_z, slot):
        return remote(
            far_out.at[i, u],
            far_in.at[i, slot, u],
            far_send,
            far_recv.at[i, slot, u],
            (at(device_z, x), tp),
        )

    def spread(i, u):
        for dx in range(1, nx):
            x_copies[i, dx, u].wait_recv()
        total = row_sums[i, u]
        for dx in range(1, nx):
            total += x_in[i, dx - 1, u].astype(f32)
        row_sums[i, u] = total
        if u < span:

            @pl.when(z != gate_way)
            def _():
                far_out[i, u] = total.astype(bf16)
                far_copy(i, u, gate_way, local).start()

        elif u in mates:
            m = u - span + 1
            near_out[i, m - 1] = total.astype(bf16)
            near_copies[i, m] = push(
                near_out.at[i, m - 1],
                near_in.at[i, m - 1],
                near_send,
                near_recv.at[i, m - 1],
                (at(near(m), x), tp),
            )

    def cross(i, u):
        @pl.when(z == gate_way)
        def _():
            total = row_sums[i, u]
            for m in range(1, span):
                slot = lax.rem(local + m, span)
                far_copy(i, u, near(m), slot).wait_recv()
                total += far_in[i, slot, u].astype(f32)
            cross_out[i, u] = total.astype(bf16)
            push(
                cross_out.at[i, u],
                cross_in.at[i],
                cross_send,
                cross_recv.at[i],
                (at(units[u], x), tp),
            )

    def finish(i):
        total = row_sums[i, own_unit]
        for m in range(1, span):
            near_copies[i, m].wait_recv()
            total += near_in[i, m - 1].astype(f32)
        bulk(cross_in.at[i], cross_send, cross_recv.at[i]).wait_recv()
        total += cross_in[i].astype(f32)
        finished[:, i * LANES : (i + 1) * LANES] = total.astype(bf16)

    far_units, all_units = range(span), range(nz)

    def each(stage, i, which):
        if 0 <= i < chunks:
            for u in which:
                stage(i, u)

    for step in range(chunks):
        project(step)
        each(spread, step - 2, all_units)
        each(combine, step - 1, all_units)
    last = chunks - 1
    for u in all_units:
        combine(last, u)
        if last > 0:
            spread(last - 1, u)
        if u == span - 1:
            for i in range(last - 1):
                each(cross, i, far_units)
        if u >= span:
            spread(last, u - span)
    each(cross, last - 1, far_units)
    for u in range(nz - span, nz):
        cross(last, u - nz + span)
        spread(last, u)
    for i in range(chunks):
        finish(i)

    column_to = lax.broadcasted_iota(jnp.int32, (part, part), 1)
    share_to = column_to // source_rows
    inner_to = lax.rem(column_to, source_rows)
    from_to = (inner_to // piece) * LANES + share_to * piece + lax.rem(inner_to, piece)
    order = (lax.broadcasted_iota(jnp.int32, (part, part), 0) == from_to).astype(bf16)
    out[...] = jnp.dot(finished[...], order, preferred_element_type=f32).astype(bf16)

    @pl.when(z == gate_way)
    def _():
        for i in range(span):
            relayed = gathered.at[pl.ds(0, len(beside_half))]
            bulk(relayed, relay_send.at[i], meta_recv).wait_send()
        bulk(cross_out, cross_send, meta_recv).wait_send()

    @pl.when(z != gate_way)
    def _():
        bulk(far_out, far_send, meta_recv).wait_send()

    bulk(meta.at[pl.ds(0, n - 1)], meta_send, meta_recv).wait_send()
    bulk(gathered.at[pl.ds(0, len(beside_half) + 1)], token_send, meta_recv).wait_send()
    bulk(staged, weight_send, meta_recv).wait_send()
    bulk(given, pair_send, meta_recv).wait_send()
    bulk(chip_sums, chip_send, meta_recv).wait_send()
    bulk(x_out, x_send, meta_recv).wait_send()
    bulk(near_out, near_send, meta_recv).wait_send()
    for h in range(1, chips):
        bulk(routed.at[tp], forward_send.at[h], meta_recv).wait_send()
    for copy in shared:
        copy.wait_send()


def settle_kernel(*refs):
    count = (len(refs) - 1) // 2
    sems = refs[-1]
    copies = [
        pltpu.make_async_copy(refs[i], refs[count + i], sems.at[i]) for i in range(count)
    ]
    for copy in copies:
        copy.start()
    for copy in copies:
        copy.wait()


def settle(*arrays):
    anywhere = pl.BlockSpec(memory_space=pl.ANY)
    hbm = pl.BlockSpec(memory_space=pltpu.HBM)
    return pl.pallas_call(
        settle_kernel,
        out_shape=tuple(jax.ShapeDtypeStruct(a.shape, a.dtype) for a in arrays),
        in_specs=[anywhere] * len(arrays),
        out_specs=(hbm,) * len(arrays),
        scratch_shapes=[pltpu.SemaphoreType.DMA((len(arrays),))],
        compiler_params=pltpu.CompilerParams(vmem_limit_bytes=1024 * 1024),
    )(*arrays)


def hand_over(tokens, gain, routes, route_weights, gate_local, up_local, down_local):
    n = lax.axis_size("fs")
    groups = lax.axis_size("tp")
    tok_rows, width = tokens.shape
    top_count = routes.shape[0]
    source_rows, units = gate_local.shape[1:]
    capacity = 3 * tok_rows * top_count // (2 * n)
    total_slots = n * capacity
    part = width // groups
    chips = groups // CORES
    nx = line_width(n)
    nz = n // nx
    span = nz // 2
    chunks = part // LANES
    vmem = pl.BlockSpec(memory_space=pltpu.VMEM)
    hbm = pl.BlockSpec(memory_space=pltpu.HBM)
    bf16, f32 = jnp.bfloat16, jnp.float32
    ready = jax.ShapeDtypeStruct((width, units), bf16)
    dma = pltpu.SemaphoreType.DMA
    rows = (tok_rows, LANES)
    return pl.pallas_call(
        functools.partial(kernel, n, groups, nx, total_slots // 4),
        out_shape=(ready, ready, ready, jax.ShapeDtypeStruct((tok_rows, part), bf16)),
        in_specs=[hbm] * 7,
        out_specs=(vmem,) * 4,
        scratch_shapes=[
            pltpu.VMEM((DEPTH, source_rows, units), f32),
            pltpu.VMEM((tok_rows, width), bf16),
            pltpu.VMEM((1, source_rows), f32),
            pltpu.VMEM((source_rows, 1), f32),
            pltpu.VMEM((tok_rows, 1), f32),
            pltpu.VMEM((top_count, tok_rows), jnp.int32),
            pltpu.VMEM((top_count, tok_rows), bf16),
            pltpu.VMEM((3, n - 1, source_rows, units), bf16),
            pltpu.VMEM((n, tok_rows, part), bf16),
            pltpu.VMEM((n, 8, LANES), f32),
            pltpu.VMEM((n, 8, LANES), f32),
            pltpu.VMEM((n, tok_rows, capacity), bf16),
            pltpu.VMEM((groups, total_slots, part), bf16),
            pltpu.VMEM((total_slots, units), f32),
            pltpu.VMEM((total_slots, units), bf16),
            pltpu.VMEM((chunks, chips, total_slots, LANES), bf16),
            pltpu.VMEM((chunks, chips, total_slots, LANES), bf16),
            pltpu.VMEM((chunks, chips, total_slots, LANES), bf16),
            pltpu.VMEM((chunks, chips - 1, total_slots, LANES), bf16),
            pltpu.VMEM((total_slots, LANES), bf16),
            pltpu.VMEM((chunks, nz) + rows, f32),
            pltpu.VMEM((chunks, nx - 1, nz) + rows, bf16),
            pltpu.VMEM((chunks, nx - 1, nz) + rows, bf16),
            pltpu.VMEM((chunks, span - 1) + rows, bf16),
            pltpu.VMEM((chunks, span - 1) + rows, bf16),
            pltpu.VMEM((chunks, span) + rows, bf16),
            pltpu.VMEM((chunks, span, span) + rows, bf16),
            pltpu.VMEM((chunks, span) + rows, bf16),
            pltpu.VMEM((chunks,) + rows, bf16),
            pltpu.VMEM((tok_rows, part), bf16),
            dma((DEPTH,)),
            dma((5,)),
            dma,
            dma,
            dma,
            dma((span,)),
            dma((n,)),
            dma((chips,)),
            dma((chips,)),
            dma((chips,)),
            dma((chips,)),
            dma,
            dma((2,)),
            dma((chunks,)),
            dma,
            dma((chunks, nz)),
            dma,
            dma((chunks, chips, nz)),
            dma,
            dma((chunks, nx, nz)),
            dma,
            dma((chunks, span - 1)),
            dma,
            dma((chunks, span, span)),
            dma,
            dma((chunks,)),
        ],
        compiler_params=pltpu.CompilerParams(
            collective_id=0, has_side_effects=True, vmem_limit_bytes=44 * 1024 * 1024
        ),
    )(
        *(
            pltpu.with_memory_space_constraint(a, pltpu.HBM)
            for a in (tokens, gain, routes, route_weights, gate_local, up_local, down_local)
        )
    )


def body(tokens, norm_gain, gate_weight, up_weight, down_weight, routes, route_weights):
    gate_ready, up_ready, down_ready, moe_output = hand_over(
        tokens,
        norm_gain[None, :],
        routes.T,
        route_weights.T,
        gate_weight,
        up_weight,
        down_weight,
    )
    return settle(gate_ready[None], up_ready[None], down_ready[None], moe_output)


def solution(mesh):
    in_specs = (
        P("fs", None),
        P("fs"),
        P(None, "fs", "tp"),
        P(None, "fs", "tp"),
        P(None, "fs", "tp"),
        P("fs", None),
        P("fs", None),
    )
    out_specs = (P("fs", None, "tp"), P("fs", None, "tp"), P("fs", None, "tp"), P("fs", "tp"))
    return jax.shard_map(body, mesh=mesh, in_specs=in_specs, out_specs=out_specs, check_vma=False)
```

```python
import functools

import jax
import jax.numpy as jnp
from jax import lax
from jax.experimental import pallas as pl
from jax.experimental.pallas import tpu as pltpu
from jax.sharding import PartitionSpec as P

norm_eps = 1e-06
clamp_limit = 7.0
gate_alpha = 1.702
MESH = pl.DeviceIdType.MESH
CORES = 2
DEPTH = 6
LANES = 128


def activate(gate_pre, up_pre):
    gate_part = jnp.minimum(gate_pre, clamp_limit)
    up_part = jnp.clip(up_pre, -clamp_limit, clamp_limit)
    return (up_part + 1.0) * gate_part * jax.nn.sigmoid(gate_alpha * gate_part)


def line_width(n):
    width = 1
    while 4 * width * width <= n:
        width *= 2
    return width


def kernel(
    n,
    groups,
    nx,
    row_tile,
    tokens,
    gain_in,
    routes_in,
    route_weights_in,
    gate_local,
    up_local,
    down_local,
    gate_ready,
    up_ready,
    down_ready,
    out,
    wide,
    token_rows,
    gain_row,
    gain,
    scale,
    routes,
    route_weights,
    staged,
    gathered,
    meta,
    metas,
    tables,
    routed,
    gate_pre,
    hidden,
    given,
    kept,
    partner_sums,
    chip_sums,
    expert_out,
    row_sums,
    x_out,
    x_in,
    near_out,
    near_in,
    far_out,
    far_in,
    cross_out,
    cross_in,
    finished,
    wide_sem,
    input_sem,
    meta_send,
    meta_recv,
    token_send,
    relay_send,
    token_recv,
    share_send,
    share_recv,
    forward_send,
    forward_recv,
    weight_send,
    weight_recv,
    down_recv,
    pair_send,
    pair_recv,
    chip_send,
    chip_recv,
    x_send,
    x_recv,
    near_send,
    near_recv,
    far_send,
    far_recv,
    cross_send,
    cross_recv,
):
    me = lax.axis_index("fs")
    tp = lax.axis_index("tp")
    chips = groups // CORES
    chip = tp // CORES
    core = lax.rem(tp, CORES)
    partner = chip * CORES + (CORES - 1 - core)
    nz = n // nx
    span = nz // 2
    z = me // nx
    x = lax.rem(me, nx)
    half = z // span
    local = lax.rem(z, span)
    gate_way = span - 1 + half
    far_way = span - half
    tok_rows, width = token_rows.shape
    part = width // groups
    source_rows = gate_local.shape[1]
    shares = n // groups
    total_slots = hidden.shape[0]
    capacity = total_slots // n
    chunks = given.shape[0]
    piece = source_rows // chunks
    f32, bf16 = jnp.float32, jnp.bfloat16

    def at(zz, xx):
        return zz * nx + xx

    def near(i):
        return half * span + lax.rem(local + i, span)

    def far(i):
        return (1 - half) * span + lax.rem(local + i, span)

    def beside(dx):
        return lax.rem(x + dx, nx)

    def slots_of(block):
        return pl.ds(pl.multiple_of(block * capacity, 16), capacity)

    def rows_of(block):
        return pl.ds(pl.multiple_of(block * source_rows, 16), source_rows)

    def chunk_of(block, i):
        return pl.ds(pl.multiple_of(block * source_rows + i * piece, 16), piece)

    group_rows = nx * capacity
    lane_rows = tok_rows // LANES

    def remote(src, dst, send_sem, recv_sem, device):
        return pltpu.make_async_remote_copy(
            src_ref=src,
            dst_ref=dst,
            send_sem=send_sem,
            recv_sem=recv_sem,
            device_id=device,
            device_id_type=MESH,
        )

    def push(src, dst, send_sem, recv_sem, device):
        copy = remote(src, dst, send_sem, recv_sem, device)
        copy.start()
        return copy

    def bulk(ref, send_sem, recv_sem):
        return remote(ref, ref, send_sem, recv_sem, (me, partner))

    peers = [at(far(i), beside(dx)) for dx in range(nx) for i in range(span)]
    peers += [at(near(i), beside(dx)) for dx in range(nx) for i in range(span) if i + dx > 0]
    places = peers + [me]
    locals_ = (gate_local, up_local, down_local)
    readies = (gate_ready, up_ready, down_ready)
    blocks = [(j, q) for j in range(3) for q in range(n)]

    def fetch(i):
        j, q = blocks[i]
        copy = pltpu.make_async_copy(
            locals_[j].at[places[q]], wide.at[i % DEPTH], wide_sem.at[i % DEPTH]
        )
        copy.start()
        return copy

    inputs = [
        pltpu.make_async_copy(src, dst, input_sem.at[spot])
        for spot, (src, dst) in enumerate(
            (
                (gain_in, gain_row),
                (tokens, token_rows),
                (routes_in, routes),
                (route_weights_in, route_weights),
            )
        )
    ]
    own_columns = pl.ds(pl.multiple_of(tp * part, LANES), part)
    inputs.append(
        pltpu.make_async_copy(tokens.at[:, own_columns], gathered.at[me], input_sem.at[4])
    )
    for copy in inputs:
        copy.start()
    fetches = [fetch(i) for i in range(DEPTH)]

    barrier = pltpu.get_barrier_semaphore()
    for k in range(1, n):
        pl.semaphore_signal(
            barrier, inc=1, device_id=(lax.rem(me + k, n), tp), device_id_type=MESH
        )
    for k in range(1, groups):
        pl.semaphore_signal(
            barrier, inc=1, device_id=(me, lax.rem(tp + k, groups)), device_id_type=MESH
        )

    inputs[0].wait()
    gain_at = lax.broadcasted_iota(jnp.int32, (source_rows, source_rows), 0) == (
        lax.broadcasted_iota(jnp.int32, (source_rows, source_rows), 1)
    )
    gain[...] = jnp.sum(jnp.where(gain_at, gain_row[...], 0.0), axis=1, keepdims=True)

    def push_weights(j, q):
        push(
            staged.at[j, q],
            readies[j].at[rows_of(me)],
            weight_send,
            weight_recv.at[j],
            (places[q], tp),
        )

    def convert(i):
        j, q = blocks[i]
        fetches[i].wait()
        value = wide[i % DEPTH]
        if j < 2:
            value = gain[...] * value
        if q == n - 1:
            readies[j][rows_of(me), :] = value.astype(bf16)
        else:
            staged[j, q] = value.astype(bf16)
        if i + DEPTH < len(blocks):
            fetches.append(fetch(i + DEPTH))

    pl.semaphore_wait(barrier, n + groups - 2)

    def push_tokens(block, device_z, device_x):
        push(
            tokens.at[:, own_columns],
            gathered.at[block],
            token_send,
            token_recv.at[block],
            (at(device_z, device_x), tp),
        )

    beside_half = [(i, dx) for dx in range(nx) for i in range(span) if i + dx > 0]
    push_tokens(me, far_way, x)
    for i, dx in beside_half:
        push_tokens(me, near(i), beside(dx))
    convert(0)
    for copy in inputs[1:]:
        copy.wait()

    @pl.loop(0, tok_rows // 32)
    def _(tile):
        rows = pl.ds(pl.multiple_of(tile * 32, 32), 32)
        wide_rows = token_rows[rows, :].astype(f32)
        scale[rows, :] = lax.rsqrt(
            jnp.mean(wide_rows * wide_rows, axis=1, keepdims=True) + norm_eps
        )

    ids = lax.broadcasted_iota(jnp.int32, (n, tok_rows), 0)
    member = jnp.zeros((n, tok_rows), f32)
    row_weight = jnp.zeros((n, tok_rows), f32)
    given_weights = route_weights[...].astype(f32)
    for k in range(routes.shape[0]):
        hit = routes[k : k + 1, :] == ids
        member += jnp.where(hit, 1.0, 0.0)
        row_weight += jnp.where(hit, given_weights[k : k + 1, :], 0.0)
    down_index = lax.broadcasted_iota(jnp.int32, (tok_rows, tok_rows), 0)
    across_index = lax.broadcasted_iota(jnp.int32, (tok_rows, tok_rows), 1)
    before = down_index < across_index
    diagonal = down_index == across_index
    scale_row = jnp.sum(jnp.where(diagonal, scale[...], 0.0), axis=0, keepdims=True)
    counts = jnp.dot(member.astype(bf16), before.astype(bf16), preferred_element_type=f32)
    position = jnp.where(member > 0.0, counts, -1.0)
    meta[...] = jnp.zeros(meta.shape, f32)
    for e in range(n):
        for r in range(lane_rows):
            lanes = slice(r * LANES, (r + 1) * LANES)
            meta[e, r : r + 1, :] = position[e : e + 1, lanes]
            meta[e, lane_rows + r : lane_rows + r + 1, :] = row_weight[e : e + 1, lanes]
            meta[e, 2 * lane_rows + r : 2 * lane_rows + r + 1, :] = scale_row[:, lanes]
    metas[me] = meta[me]

    for k in range(1, n):
        peer = lax.rem(me + k, n)
        push(meta.at[peer], metas.at[me], meta_send, meta_recv, (peer, tp))

    for q in range(1, n):
        convert(q)
        if q <= span:
            push_weights(0, q - 1)
    for q in range(n):
        convert(n + q)

    def push_rest():
        for q in range(span, n - 1):
            push_weights(0, q)

    def push_up():
        for q in range(n - 1):
            push_weights(1, q)

    @pl.when(z != gate_way)
    def _():
        push_rest()
        push_up()

    bulk(metas.at[pl.ds(0, n - 1)], meta_send, meta_recv).wait_recv()

    def await_tokens(block):
        bulk(gathered.at[block], token_send, token_recv.at[block]).wait_recv()

    def share_block(block):
        def to(step, device):
            remote(
                routed.at[tp, slots_of(block)],
                routed.at[tp, slots_of(block)],
                share_send.at[step],
                share_recv.at[step],
                (me, device),
            ).start()

        for h in range(1, chips):
            to(h, lax.rem(chip + h, chips) * CORES + core)
        to(0, partner)

    lines = lax.broadcasted_iota(jnp.int32, (capacity, tok_rows), 0).astype(f32)
    columns_of = lax.broadcasted_iota(jnp.int32, (tok_rows, capacity), 1).astype(f32)
    pending = []

    def pick(block):
        found = metas[block]
        place, weight, scale_across = (
            jnp.concatenate([found[j + r : j + r + 1, :] for r in range(lane_rows)], axis=1)
            for j in (0, lane_rows, 2 * lane_rows)
        )
        chosen = jnp.where(place == lines, 1.0, 0.0).astype(bf16)
        scale_down = jnp.sum(jnp.where(diagonal, scale_across, 0.0), axis=1, keepdims=True)
        normed = (gathered[block].astype(f32) * scale_down).astype(bf16)
        routed[tp, slots_of(block), :] = jnp.dot(
            chosen, normed, preferred_element_type=f32
        ).astype(bf16)
        if pending:
            share_block(pending.pop())
        ones = jnp.ones((tok_rows, capacity), bf16)
        place_down = jnp.dot(
            jnp.where(diagonal, place, 0.0).astype(bf16), ones, preferred_element_type=f32
        )
        weight_down = jnp.dot(
            jnp.where(diagonal, weight, 0.0).astype(bf16), ones, preferred_element_type=f32
        )
        tables[block] = jnp.where(place_down == columns_of, weight_down, 0.0).astype(bf16)
        pending.append(block)

    pick(me)
    for i, dx in beside_half:
        block = at(near(i), beside(dx))
        await_tokens(block)
        pick(block)
    for i in range(span):
        block = at(far(i), x)
        await_tokens(block)

        @pl.when(z == gate_way)
        def _(i=i, block=block):
            for m, dx in beside_half:
                push(
                    gathered.at[block],
                    gathered.at[block],
                    relay_send.at[i],
                    token_recv.at[block],
                    (at(near(m), beside(dx)), tp),
                )

    pl.when(z == gate_way)(push_rest)
    for dx in range(nx):
        for i in range(span):
            block = at(far(i), beside(dx))
            if dx > 0:
                await_tokens(block)
            pick(block)
    share_block(pending.pop())

    pl.when(z == gate_way)(push_up)
    for q in range(n):
        convert(2 * n + q)

    def all_rows(step, origin, device):
        return remote(
            routed.at[tp], routed.at[origin], share_send.at[step], share_recv.at[step], (me, device)
        )

    shared = []
    for h in range(1, chips):
        origin = lax.rem(chip - h + chips, chips) * CORES + core
        copy = all_rows(h, origin, partner)
        copy.wait_recv()
        shared.append(copy)
        push(
            routed.at[origin],
            routed.at[origin],
            forward_send.at[h],
            forward_recv.at[h],
            (me, partner),
        )
    copy = all_rows(0, partner, partner)
    copy.wait_recv()
    shared.append(copy)
    for h in range(1, chips):
        origin = lax.rem(chip - h + chips, chips) * CORES + (CORES - 1 - core)
        remote(
            routed.at[origin],
            routed.at[origin],
            forward_send.at[h],
            forward_recv.at[h],
            (me, partner),
        ).wait_recv()

    def await_weights(j):
        received = readies[j].at[pl.ds(0, (n - 1) * source_rows)]
        bulk(received, weight_send, weight_recv.at[j]).wait_recv()

    def product(rows, ready):
        total = jnp.zeros((row_tile, hidden.shape[1]), f32)
        for t in range(groups):
            total += jnp.dot(
                routed[t, rows, :],
                ready[t * part : (t + 1) * part],
                preferred_element_type=f32,
            )
        return total

    def tiles(body):
        @pl.loop(0, total_slots // row_tile)
        def _(tile):
            body(pl.ds(pl.multiple_of(tile * row_tile, 16), row_tile))

    await_weights(0)

    @tiles
    def _(rows):
        gate_pre[rows, :] = product(rows, gate_ready)

    def push_down(i):
        for q in range(n - 1):
            push(
                staged.at[2, q, pl.ds(i * piece, piece)],
                down_ready.at[chunk_of(me, i)],
                weight_send,
                down_recv.at[i],
                (places[q], tp),
            )

    @pl.when(z == gate_way)
    def _():
        for i in range(chunks):
            push_down(i)

    await_weights(1)
    pl.when(z != gate_way)(functools.partial(push_down, 0))

    @tiles
    def _(rows):
        hidden[rows, :] = activate(gate_pre[rows, :], product(rows, up_ready)).astype(bf16)

    over_copies = {}
    units = [(1 - half) * span + f for f in range(span)]
    units += [near(m) for m in range(1, span)] + [z]
    mates = range(span, nz - 1)
    own_unit = nz - 1

    def rows_in(u):
        return pl.ds(pl.multiple_of(units[u] * group_rows, 16), group_rows)

    def project(i):
        received = down_ready.at[pl.ds(0, (n - 1) * piece)]
        bulk(received, weight_send, down_recv.at[i]).wait_recv()
        if i + 1 < chunks:
            pl.when(z != gate_way)(functools.partial(push_down, i + 1))

        def rows_to(side):
            picked = [
                down_ready[
                    chunk_of((lax.rem(chip + h, chips) * CORES + side) * shares + r, i), :
                ]
                for h in range(chips)
                for r in range(shares)
            ]
            return jnp.concatenate(picked, axis=0)

        def run(down, target, u):
            rows = rows_in(u)
            value = lax.dot_general(
                hidden[rows, :], down, (((1,), (1,)), ((), ())), preferred_element_type=f32
            ).astype(bf16)
            for h in range(chips):
                target[i, h, rows, :] = value[:, h * LANES : (h + 1) * LANES]

        give = rows_to(CORES - 1 - core)
        for u in range(nz):
            run(give, given, u)
            for h in range(chips):
                push(
                    given.at[i, h, rows_in(u)],
                    partner_sums.at[i, h, rows_in(u)],
                    pair_send,
                    pair_recv.at[i, u],
                    (me, partner),
                )
        keep = rows_to(core)
        for u in range(nz):
            rows = rows_in(u)
            run(keep, kept, u)
            bulk(given.at[i, pl.ds(0, chips), rows], pair_send, pair_recv.at[i, u]).wait_recv()
            for h in range(1, chips):
                total = kept[i, h, rows, :].astype(f32)
                total += partner_sums[i, h, rows, :].astype(f32)
                kept[i, h, rows, :] = total.astype(bf16)
                over_copies[i, h, u] = push(
                    kept.at[i, h, rows],
                    chip_sums.at[i, h - 1, rows],
                    chip_send,
                    chip_recv.at[i, h - 1, u],
                    (me, lax.rem(chip + h, chips) * CORES + core),
                )

    x_copies = {}

    def combine(i, u):
        for h in range(1, chips):
            over_copies[i, h, u].wait_recv()

        rows = rows_in(u)
        total = kept[i, 0, rows, :].astype(f32) + partner_sums[i, 0, rows, :].astype(f32)
        for h in range(1, chips):
            total += chip_sums[i, h - 1, rows, :].astype(f32)
        expert_out[rows, :] = total.astype(bf16)

        def rows_for(xx):
            block = at(units[u], xx)
            return jnp.dot(
                tables[block], expert_out[slots_of(block), :], preferred_element_type=f32
            )

        for dx in range(1, nx):
            x_out[i, dx - 1, u] = rows_for(beside(dx)).astype(bf16)
            x_copies[i, dx, u] = push(
                x_out.at[i, dx - 1, u],
                x_in.at[i, dx - 1, u],
                x_send,
                x_recv.at[i, dx - 1, u],
                (at(z, beside(dx)), tp),
            )
        row_sums[i, u] = rows_for(x)

    near_copies = {}

    def far_copy(i, u, device_z, slot):
        return remote(
            far_out.at[i, u],
            far_in.at[i, slot, u],
            far_send,
            far_recv.at[i, slot, u],
            (at(device_z, x), tp),
        )

    def spread(i, u):
        for dx in range(1, nx):
            x_copies[i, dx, u].wait_recv()
        total = row_sums[i, u]
        for dx in range(1, nx):
            total += x_in[i, dx - 1, u].astype(f32)
        row_sums[i, u] = total
        if u < span:

            @pl.when(z != gate_way)
            def _():
                far_out[i, u] = total.astype(bf16)
                far_copy(i, u, gate_way, local).start()

        elif u in mates:
            m = u - span + 1
            near_out[i, m - 1] = total.astype(bf16)
            near_copies[i, m] = push(
                near_out.at[i, m - 1],
                near_in.at[i, m - 1],
                near_send,
                near_recv.at[i, m - 1],
                (at(near(m), x), tp),
            )

    def cross(i, u):
        @pl.when(z == gate_way)
        def _():
            total = row_sums[i, u]
            for m in range(1, span):
                slot = lax.rem(local + m, span)
                far_copy(i, u, near(m), slot).wait_recv()
                total += far_in[i, slot, u].astype(f32)
            cross_out[i, u] = total.astype(bf16)
            push(
                cross_out.at[i, u],
                cross_in.at[i],
                cross_send,
                cross_recv.at[i],
                (at(units[u], x), tp),
            )

    def finish(i):
        total = row_sums[i, own_unit]
        for m in range(1, span):
            near_copies[i, m].wait_recv()
            total += near_in[i, m - 1].astype(f32)
        bulk(cross_in.at[i], cross_send, cross_recv.at[i]).wait_recv()
        total += cross_in[i].astype(f32)
        finished[:, i * LANES : (i + 1) * LANES] = total.astype(bf16)

    far_units, all_units = range(span), range(nz)

    def each(stage, i, which):
        if 0 <= i < chunks:
            for u in which:
                stage(i, u)

    last = chunks - 1
    near_units = range(span, nz)
    for step in range(chunks):
        if step == last:
            each(combine, step - 1, far_units)
        project(step)
        each(combine, step - 1, all_units if step < last else near_units)
        each(spread, step - 2, far_units)
        if step == last:
            for i in range(last - 2):
                each(cross, i, far_units)
        each(spread, step - 2, near_units)
    for u in far_units:
        combine(last, u)
        each(spread, last - 1, [u])
        if u == 0:
            each(cross, last - 2, far_units)
    for u in near_units:
        if u == nz - 1:
            spread(last, 0)
        combine(last, u)
        if u - span < span:
            each(cross, last - 1, [u - span])
        each(spread, last - 1, [u] if u < nz - 1 else [])
    for u in range(1, nz):
        spread(last, u)
        if u == 1:
            each(spread, last - 1, [nz - 1])
        if u - 1 < span:
            cross(last, u - 1)
    for i in range(chunks):
        finish(i)

    column_to = lax.broadcasted_iota(jnp.int32, (part, part), 1)
    share_to = column_to // source_rows
    inner_to = lax.rem(column_to, source_rows)
    from_to = (inner_to // piece) * LANES + share_to * piece + lax.rem(inner_to, piece)
    order = (lax.broadcasted_iota(jnp.int32, (part, part), 0) == from_to).astype(bf16)
    out[...] = jnp.dot(finished[...], order, preferred_element_type=f32).astype(bf16)

    @pl.when(z == gate_way)
    def _():
        for i in range(span):
            relayed = gathered.at[pl.ds(0, len(beside_half))]
            bulk(relayed, relay_send.at[i], meta_recv).wait_send()
        bulk(cross_out, cross_send, meta_recv).wait_send()

    @pl.when(z != gate_way)
    def _():
        bulk(far_out, far_send, meta_recv).wait_send()

    bulk(meta.at[pl.ds(0, n - 1)], meta_send, meta_recv).wait_send()
    bulk(gathered.at[pl.ds(0, len(beside_half) + 1)], token_send, meta_recv).wait_send()
    bulk(staged, weight_send, meta_recv).wait_send()
    bulk(given, pair_send, meta_recv).wait_send()
    bulk(chip_sums, chip_send, meta_recv).wait_send()
    bulk(x_out, x_send, meta_recv).wait_send()
    bulk(near_out, near_send, meta_recv).wait_send()
    for h in range(1, chips):
        bulk(routed.at[tp], forward_send.at[h], meta_recv).wait_send()
    for copy in shared:
        copy.wait_send()


def settle_kernel(*refs):
    count = (len(refs) - 1) // 2
    sems = refs[-1]
    copies = [
        pltpu.make_async_copy(refs[i], refs[count + i], sems.at[i]) for i in range(count)
    ]
    for copy in copies:
        copy.start()
    for copy in copies:
        copy.wait()


def settle(*arrays):
    anywhere = pl.BlockSpec(memory_space=pl.ANY)
    hbm = pl.BlockSpec(memory_space=pltpu.HBM)
    return pl.pallas_call(
        settle_kernel,
        out_shape=tuple(jax.ShapeDtypeStruct(a.shape, a.dtype) for a in arrays),
        in_specs=[anywhere] * len(arrays),
        out_specs=(hbm,) * len(arrays),
        scratch_shapes=[pltpu.SemaphoreType.DMA((len(arrays),))],
        compiler_params=pltpu.CompilerParams(vmem_limit_bytes=1024 * 1024),
    )(*arrays)


def hand_over(tokens, gain, routes, route_weights, gate_local, up_local, down_local):
    n = lax.axis_size("fs")
    groups = lax.axis_size("tp")
    tok_rows, width = tokens.shape
    top_count = routes.shape[0]
    source_rows, units = gate_local.shape[1:]
    capacity = 3 * tok_rows * top_count // (2 * n)
    total_slots = n * capacity
    part = width // groups
    chips = groups // CORES
    nx = line_width(n)
    nz = n // nx
    span = nz // 2
    chunks = part // LANES
    vmem = pl.BlockSpec(memory_space=pltpu.VMEM)
    hbm = pl.BlockSpec(memory_space=pltpu.HBM)
    bf16, f32 = jnp.bfloat16, jnp.float32
    ready = jax.ShapeDtypeStruct((width, units), bf16)
    dma = pltpu.SemaphoreType.DMA
    rows = (tok_rows, LANES)
    return pl.pallas_call(
        functools.partial(kernel, n, groups, nx, total_slots // 4),
        out_shape=(ready, ready, ready, jax.ShapeDtypeStruct((tok_rows, part), bf16)),
        in_specs=[hbm] * 7,
        out_specs=(vmem,) * 4,
        scratch_shapes=[
            pltpu.VMEM((DEPTH, source_rows, units), f32),
            pltpu.VMEM((tok_rows, width), bf16),
            pltpu.VMEM((1, source_rows), f32),
            pltpu.VMEM((source_rows, 1), f32),
            pltpu.VMEM((tok_rows, 1), f32),
            pltpu.VMEM((top_count, tok_rows), jnp.int32),
            pltpu.VMEM((top_count, tok_rows), bf16),
            pltpu.VMEM((3, n - 1, source_rows, units), bf16),
            pltpu.VMEM((n, tok_rows, part), bf16),
            pltpu.VMEM((n, 8, LANES), f32),
            pltpu.VMEM((n, 8, LANES), f32),
            pltpu.VMEM((n, tok_rows, capacity), bf16),
            pltpu.VMEM((groups, total_slots, part), bf16),
            pltpu.VMEM((total_slots, units), f32),
            pltpu.VMEM((total_slots, units), bf16),
            pltpu.VMEM((chunks, chips, total_slots, LANES), bf16),
            pltpu.VMEM((chunks, chips, total_slots, LANES), bf16),
            pltpu.VMEM((chunks, chips, total_slots, LANES), bf16),
            pltpu.VMEM((chunks, chips - 1, total_slots, LANES), bf16),
            pltpu.VMEM((total_slots, LANES), bf16),
            pltpu.VMEM((chunks, nz) + rows, f32),
            pltpu.VMEM((chunks, nx - 1, nz) + rows, bf16),
            pltpu.VMEM((chunks, nx - 1, nz) + rows, bf16),
            pltpu.VMEM((chunks, span - 1) + rows, bf16),
            pltpu.VMEM((chunks, span - 1) + rows, bf16),
            pltpu.VMEM((chunks, span) + rows, bf16),
            pltpu.VMEM((chunks, span, span) + rows, bf16),
            pltpu.VMEM((chunks, span) + rows, bf16),
            pltpu.VMEM((chunks,) + rows, bf16),
            pltpu.VMEM((tok_rows, part), bf16),
            dma((DEPTH,)),
            dma((5,)),
            dma,
            dma,
            dma,
            dma((span,)),
            dma((n,)),
            dma((chips,)),
            dma((chips,)),
            dma((chips,)),
            dma((chips,)),
            dma,
            dma((2,)),
            dma((chunks,)),
            dma,
            dma((chunks, nz)),
            dma,
            dma((chunks, chips - 1, nz)),
            dma,
            dma((chunks, nx - 1, nz)),
            dma,
            dma((chunks, span - 1)),
            dma,
            dma((chunks, span, span)),
            dma,
            dma((chunks,)),
        ],
        compiler_params=pltpu.CompilerParams(
            collective_id=0, has_side_effects=True, vmem_limit_bytes=44 * 1024 * 1024
        ),
    )(
        *(
            pltpu.with_memory_space_constraint(a, pltpu.HBM)
            for a in (tokens, gain, routes, route_weights, gate_local, up_local, down_local)
        )
    )


def body(tokens, norm_gain, gate_weight, up_weight, down_weight, routes, route_weights):
    gate_ready, up_ready, down_ready, moe_output = hand_over(
        tokens,
        norm_gain[None, :],
        routes.T,
        route_weights.T,
        gate_weight,
        up_weight,
        down_weight,
    )
    return settle(gate_ready[None], up_ready[None], down_ready[None], moe_output)


def solution(mesh):
    in_specs = (
        P("fs", None),
        P("fs"),
        P(None, "fs", "tp"),
        P(None, "fs", "tp"),
        P(None, "fs", "tp"),
        P("fs", None),
        P("fs", None),
    )
    out_specs = (P("fs", None, "tp"), P("fs", None, "tp"), P("fs", None, "tp"), P("fs", "tp"))
    return jax.shard_map(body, mesh=mesh, in_specs=in_specs, out_specs=out_specs, check_vma=False)
```

```python
import functools

import jax
import jax.numpy as jnp
from jax import lax
from jax.experimental import pallas as pl
from jax.experimental.pallas import tpu as pltpu
from jax.sharding import PartitionSpec as P

norm_eps = 1e-06
clamp_limit = 7.0
gate_alpha = 1.702
MESH = pl.DeviceIdType.MESH
CORES = 2
DEPTH = 6
LANES = 128


def activate(gate_pre, up_pre):
    gate_part = jnp.minimum(gate_pre, clamp_limit)
    up_part = jnp.clip(up_pre, -clamp_limit, clamp_limit)
    return (up_part + 1.0) * gate_part * jax.nn.sigmoid(gate_alpha * gate_part)


def line_width(n):
    width = 1
    while 4 * width * width <= n:
        width *= 2
    return width


def kernel(
    n,
    groups,
    nx,
    row_tile,
    tokens,
    gain_in,
    routes_in,
    route_weights_in,
    gate_local,
    up_local,
    down_local,
    gate_ready,
    up_ready,
    down_ready,
    out,
    wide,
    token_rows,
    gain_row,
    gain,
    scale,
    routes,
    route_weights,
    staged,
    gathered,
    meta,
    metas,
    tables,
    routed,
    gate_pre,
    hidden,
    given,
    kept,
    partner_sums,
    chip_sums,
    expert_out,
    row_sums,
    x_out,
    x_in,
    near_out,
    near_in,
    far_out,
    far_in,
    cross_out,
    cross_in,
    finished,
    wide_sem,
    input_sem,
    meta_send,
    meta_recv,
    token_send,
    relay_send,
    token_recv,
    share_send,
    share_recv,
    forward_send,
    forward_recv,
    weight_send,
    weight_recv,
    down_recv,
    pair_send,
    pair_recv,
    chip_send,
    chip_recv,
    x_send,
    x_recv,
    near_send,
    near_recv,
    far_send,
    far_recv,
    cross_send,
    cross_recv,
):
    me = lax.axis_index("fs")
    tp = lax.axis_index("tp")
    chips = groups // CORES
    chip = tp // CORES
    core = lax.rem(tp, CORES)
    partner = chip * CORES + (CORES - 1 - core)
    nz = n // nx
    span = nz // 2
    z = me // nx
    x = lax.rem(me, nx)
    half = z // span
    local = lax.rem(z, span)
    gate_way = span - 1 + half
    far_way = span - half
    tok_rows, width = token_rows.shape
    part = width // groups
    source_rows = gate_local.shape[1]
    shares = n // groups
    total_slots = hidden.shape[0]
    capacity = total_slots // n
    chunks = given.shape[0]
    piece = source_rows // chunks
    f32, bf16 = jnp.float32, jnp.bfloat16

    def at(zz, xx):
        return zz * nx + xx

    def near(i):
        return half * span + lax.rem(local + i, span)

    def far(i):
        return (1 - half) * span + lax.rem(local + i, span)

    def beside(dx):
        return lax.rem(x + dx, nx)

    def slots_of(block):
        return pl.ds(pl.multiple_of(block * capacity, 16), capacity)

    def rows_of(block):
        return pl.ds(pl.multiple_of(block * source_rows, 16), source_rows)

    def chunk_of(block, i):
        return pl.ds(pl.multiple_of(block * source_rows + i * piece, 16), piece)

    group_rows = nx * capacity
    lane_rows = tok_rows // LANES

    def remote(src, dst, send_sem, recv_sem, device):
        return pltpu.make_async_remote_copy(
            src_ref=src,
            dst_ref=dst,
            send_sem=send_sem,
            recv_sem=recv_sem,
            device_id=device,
            device_id_type=MESH,
        )

    def push(src, dst, send_sem, recv_sem, device):
        copy = remote(src, dst, send_sem, recv_sem, device)
        copy.start()
        return copy

    def bulk(ref, send_sem, recv_sem):
        return remote(ref, ref, send_sem, recv_sem, (me, partner))

    peers = [at(far(i), beside(dx)) for dx in range(nx) for i in range(span)]
    peers += [at(near(i), beside(dx)) for dx in range(nx) for i in range(span) if i + dx > 0]
    places = peers + [me]
    locals_ = (gate_local, up_local, down_local)
    readies = (gate_ready, up_ready, down_ready)
    blocks = [(j, q) for j in range(3) for q in range(n)]

    def fetch(i):
        j, q = blocks[i]
        copy = pltpu.make_async_copy(
            locals_[j].at[places[q]], wide.at[i % DEPTH], wide_sem.at[i % DEPTH]
        )
        copy.start()
        return copy

    inputs = [
        pltpu.make_async_copy(src, dst, input_sem.at[spot])
        for spot, (src, dst) in enumerate(
            (
                (gain_in, gain_row),
                (tokens, token_rows),
                (routes_in, routes),
                (route_weights_in, route_weights),
            )
        )
    ]
    own_columns = pl.ds(pl.multiple_of(tp * part, LANES), part)
    inputs.append(
        pltpu.make_async_copy(tokens.at[:, own_columns], gathered.at[me], input_sem.at[4])
    )
    for copy in inputs:
        copy.start()
    fetches = [fetch(i) for i in range(DEPTH)]

    barrier = pltpu.get_barrier_semaphore()
    for k in range(1, n):
        pl.semaphore_signal(
            barrier, inc=1, device_id=(lax.rem(me + k, n), tp), device_id_type=MESH
        )
    for k in range(1, groups):
        pl.semaphore_signal(
            barrier, inc=1, device_id=(me, lax.rem(tp + k, groups)), device_id_type=MESH
        )

    inputs[0].wait()
    gain_at = lax.broadcasted_iota(jnp.int32, (source_rows, source_rows), 0) == (
        lax.broadcasted_iota(jnp.int32, (source_rows, source_rows), 1)
    )
    gain[...] = jnp.sum(jnp.where(gain_at, gain_row[...], 0.0), axis=1, keepdims=True)

    def push_weights(j, q):
        push(
            staged.at[j, q],
            readies[j].at[rows_of(me)],
            weight_send,
            weight_recv.at[j],
            (places[q], tp),
        )

    def convert(i):
        j, q = blocks[i]
        fetches[i].wait()
        value = wide[i % DEPTH]
        if j < 2:
            value = gain[...] * value
        if q == n - 1:
            readies[j][rows_of(me), :] = value.astype(bf16)
        else:
            staged[j, q] = value.astype(bf16)
        if i + DEPTH < len(blocks):
            fetches.append(fetch(i + DEPTH))

    pl.semaphore_wait(barrier, n + groups - 2)

    def push_tokens(block, device_z, device_x):
        push(
            tokens.at[:, own_columns],
            gathered.at[block],
            token_send,
            token_recv.at[block],
            (at(device_z, device_x), tp),
        )

    beside_half = [(i, dx) for dx in range(nx) for i in range(span) if i + dx > 0]
    push_tokens(me, far_way, x)
    for i, dx in beside_half:
        push_tokens(me, near(i), beside(dx))
    convert(0)
    for copy in inputs[1:]:
        copy.wait()

    @pl.loop(0, tok_rows // 32)
    def _(tile):
        rows = pl.ds(pl.multiple_of(tile * 32, 32), 32)
        wide_rows = token_rows[rows, :].astype(f32)
        scale[rows, :] = lax.rsqrt(
            jnp.mean(wide_rows * wide_rows, axis=1, keepdims=True) + norm_eps
        )

    ids = lax.broadcasted_iota(jnp.int32, (n, tok_rows), 0)
    member = jnp.zeros((n, tok_rows), f32)
    row_weight = jnp.zeros((n, tok_rows), f32)
    given_weights = route_weights[...].astype(f32)
    for k in range(routes.shape[0]):
        hit = routes[k : k + 1, :] == ids
        member += jnp.where(hit, 1.0, 0.0)
        row_weight += jnp.where(hit, given_weights[k : k + 1, :], 0.0)
    down_index = lax.broadcasted_iota(jnp.int32, (tok_rows, tok_rows), 0)
    across_index = lax.broadcasted_iota(jnp.int32, (tok_rows, tok_rows), 1)
    before = down_index < across_index
    diagonal = down_index == across_index
    scale_row = jnp.sum(jnp.where(diagonal, scale[...], 0.0), axis=0, keepdims=True)
    counts = jnp.dot(member.astype(bf16), before.astype(bf16), preferred_element_type=f32)
    position = jnp.where(member > 0.0, counts, -1.0)
    meta[...] = jnp.zeros(meta.shape, f32)
    for e in range(n):
        for r in range(lane_rows):
            lanes = slice(r * LANES, (r + 1) * LANES)
            meta[e, r : r + 1, :] = position[e : e + 1, lanes]
            meta[e, lane_rows + r : lane_rows + r + 1, :] = row_weight[e : e + 1, lanes]
            meta[e, 2 * lane_rows + r : 2 * lane_rows + r + 1, :] = scale_row[:, lanes]
    metas[me] = meta[me]

    for k in range(1, n):
        peer = lax.rem(me + k, n)
        push(meta.at[peer], metas.at[me], meta_send, meta_recv, (peer, tp))

    for q in range(1, n):
        convert(q)
        if q <= span:
            push_weights(0, q - 1)
    for q in range(n):
        convert(n + q)

    def push_rest():
        for q in range(span, n - 1):
            push_weights(0, q)

    def push_up():
        for q in range(n - 1):
            push_weights(1, q)

    @pl.when(z != gate_way)
    def _():
        push_rest()
        push_up()

    bulk(metas.at[pl.ds(0, n - 1)], meta_send, meta_recv).wait_recv()

    def await_tokens(block):
        bulk(gathered.at[block], token_send, token_recv.at[block]).wait_recv()

    def share_block(block):
        def to(step, device):
            remote(
                routed.at[tp, slots_of(block)],
                routed.at[tp, slots_of(block)],
                share_send.at[step],
                share_recv.at[step],
                (me, device),
            ).start()

        for h in range(1, chips):
            to(h, lax.rem(chip + h, chips) * CORES + core)
        to(0, partner)

    lines = lax.broadcasted_iota(jnp.int32, (capacity, tok_rows), 0).astype(f32)
    columns_of = lax.broadcasted_iota(jnp.int32, (tok_rows, capacity), 1).astype(f32)
    pending = []

    def pick(block):
        found = metas[block]
        place, weight, scale_across = (
            jnp.concatenate([found[j + r : j + r + 1, :] for r in range(lane_rows)], axis=1)
            for j in (0, lane_rows, 2 * lane_rows)
        )
        chosen = jnp.where(place == lines, 1.0, 0.0).astype(bf16)
        scale_down = jnp.sum(jnp.where(diagonal, scale_across, 0.0), axis=1, keepdims=True)
        normed = (gathered[block].astype(f32) * scale_down).astype(bf16)
        routed[tp, slots_of(block), :] = jnp.dot(
            chosen, normed, preferred_element_type=f32
        ).astype(bf16)
        if pending:
            share_block(pending.pop())
        ones = jnp.ones((tok_rows, capacity), bf16)
        place_down = jnp.dot(
            jnp.where(diagonal, place, 0.0).astype(bf16), ones, preferred_element_type=f32
        )
        weight_down = jnp.dot(
            jnp.where(diagonal, weight, 0.0).astype(bf16), ones, preferred_element_type=f32
        )
        tables[block] = jnp.where(place_down == columns_of, weight_down, 0.0).astype(bf16)
        pending.append(block)

    pick(me)
    for i, dx in beside_half:
        block = at(near(i), beside(dx))
        await_tokens(block)
        pick(block)
    for i in range(span):
        block = at(far(i), x)
        await_tokens(block)

        @pl.when(z == gate_way)
        def _(i=i, block=block):
            for m, dx in beside_half:
                push(
                    gathered.at[block],
                    gathered.at[block],
                    relay_send.at[i],
                    token_recv.at[block],
                    (at(near(m), beside(dx)), tp),
                )

    pl.when(z == gate_way)(push_rest)
    for dx in range(nx):
        for i in range(span):
            block = at(far(i), beside(dx))
            if dx > 0:
                await_tokens(block)
            pick(block)
    share_block(pending.pop())

    pl.when(z == gate_way)(push_up)
    for q in range(n):
        convert(2 * n + q)

    def all_rows(step, origin, device):
        return remote(
            routed.at[tp], routed.at[origin], share_send.at[step], share_recv.at[step], (me, device)
        )

    shared = []
    for h in range(1, chips):
        origin = lax.rem(chip - h + chips, chips) * CORES + core
        copy = all_rows(h, origin, partner)
        copy.wait_recv()
        shared.append(copy)
        push(
            routed.at[origin],
            routed.at[origin],
            forward_send.at[h],
            forward_recv.at[h],
            (me, partner),
        )
    copy = all_rows(0, partner, partner)
    copy.wait_recv()
    shared.append(copy)
    for h in range(1, chips):
        origin = lax.rem(chip - h + chips, chips) * CORES + (CORES - 1 - core)
        remote(
            routed.at[origin],
            routed.at[origin],
            forward_send.at[h],
            forward_recv.at[h],
            (me, partner),
        ).wait_recv()

    def await_weights(j):
        received = readies[j].at[pl.ds(0, (n - 1) * source_rows)]
        bulk(received, weight_send, weight_recv.at[j]).wait_recv()

    def product(rows, ready):
        total = jnp.zeros((row_tile, hidden.shape[1]), f32)
        for t in range(groups):
            total += jnp.dot(
                routed[t, rows, :],
                ready[t * part : (t + 1) * part],
                preferred_element_type=f32,
            )
        return total

    def tiles(body):
        @pl.loop(0, total_slots // row_tile)
        def _(tile):
            body(pl.ds(pl.multiple_of(tile * row_tile, 16), row_tile))

    await_weights(0)

    @tiles
    def _(rows):
        gate_pre[rows, :] = product(rows, gate_ready)

    def push_down(i):
        for q in range(n - 1):
            push(
                staged.at[2, q, pl.ds(i * piece, piece)],
                down_ready.at[chunk_of(me, i)],
                weight_send,
                down_recv.at[i],
                (places[q], tp),
            )

    @pl.when(z == gate_way)
    def _():
        for i in range(chunks):
            push_down(i)

    await_weights(1)
    pl.when(z != gate_way)(functools.partial(push_down, 0))

    @tiles
    def _(rows):
        hidden[rows, :] = activate(gate_pre[rows, :], product(rows, up_ready)).astype(bf16)

    over_copies = {}
    units = [(1 - half) * span + f for f in range(span)]
    units += [near(m) for m in range(1, span)] + [z]
    mates = range(span, nz - 1)
    own_unit = nz - 1

    def rows_in(u):
        return pl.ds(pl.multiple_of(units[u] * group_rows, 16), group_rows)

    def project(i):
        received = down_ready.at[pl.ds(0, (n - 1) * piece)]
        bulk(received, weight_send, down_recv.at[i]).wait_recv()
        if i + 1 < chunks:
            pl.when(z != gate_way)(functools.partial(push_down, i + 1))

        def rows_to(side):
            picked = [
                down_ready[
                    chunk_of((lax.rem(chip + h, chips) * CORES + side) * shares + r, i), :
                ]
                for h in range(chips)
                for r in range(shares)
            ]
            return jnp.concatenate(picked, axis=0)

        def run(down, target, u):
            rows = rows_in(u)
            value = lax.dot_general(
                hidden[rows, :], down, (((1,), (1,)), ((), ())), preferred_element_type=f32
            ).astype(bf16)
            for h in range(chips):
                target[i, h, rows, :] = value[:, h * LANES : (h + 1) * LANES]

        give = rows_to(CORES - 1 - core)
        for u in range(nz):
            run(give, given, u)
            for h in range(chips):
                push(
                    given.at[i, h, rows_in(u)],
                    partner_sums.at[i, h, rows_in(u)],
                    pair_send,
                    pair_recv.at[i, u],
                    (me, partner),
                )
        keep = rows_to(core)
        for u in range(nz):
            rows = rows_in(u)
            run(keep, kept, u)
            bulk(given.at[i, pl.ds(0, chips), rows], pair_send, pair_recv.at[i, u]).wait_recv()
            for h in range(1, chips):
                total = kept[i, h, rows, :].astype(f32)
                total += partner_sums[i, h, rows, :].astype(f32)
                kept[i, h, rows, :] = total.astype(bf16)
                over_copies[i, h, u] = push(
                    kept.at[i, h, rows],
                    chip_sums.at[i, h - 1, rows],
                    chip_send,
                    chip_recv.at[i, h - 1, u],
                    (me, lax.rem(chip + h, chips) * CORES + core),
                )

    x_copies = {}

    def combine(i, u):
        for h in range(1, chips):
            over_copies[i, h, u].wait_recv()

        rows = rows_in(u)
        total = kept[i, 0, rows, :].astype(f32) + partner_sums[i, 0, rows, :].astype(f32)
        for h in range(1, chips):
            total += chip_sums[i, h - 1, rows, :].astype(f32)
        expert_out[rows, :] = total.astype(bf16)

        def rows_for(xx):
            block = at(units[u], xx)
            return jnp.dot(
                tables[block], expert_out[slots_of(block), :], preferred_element_type=f32
            )

        for dx in range(1, nx):
            x_out[i, dx - 1, u] = rows_for(beside(dx)).astype(bf16)
            x_copies[i, dx, u] = push(
                x_out.at[i, dx - 1, u],
                x_in.at[i, dx - 1, u],
                x_send,
                x_recv.at[i, dx - 1, u],
                (at(z, beside(dx)), tp),
            )
        row_sums[i, u] = rows_for(x)

    near_copies = {}

    def far_copy(i, u, device_z, slot):
        return remote(
            far_out.at[i, u],
            far_in.at[i, slot, u],
            far_send,
            far_recv.at[i, slot, u],
            (at(device_z, x), tp),
        )

    def spread(i, u):
        for dx in range(1, nx):
            x_copies[i, dx, u].wait_recv()
        total = row_sums[i, u]
        for dx in range(1, nx):
            total += x_in[i, dx - 1, u].astype(f32)
        row_sums[i, u] = total
        if u < span:

            @pl.when(z != gate_way)
            def _():
                far_out[i, u] = total.astype(bf16)
                far_copy(i, u, gate_way, local).start()

        elif u in mates:
            m = u - span + 1
            near_out[i, m - 1] = total.astype(bf16)
            near_copies[i, m] = push(
                near_out.at[i, m - 1],
                near_in.at[i, m - 1],
                near_send,
                near_recv.at[i, m - 1],
                (at(near(m), x), tp),
            )

    def cross(i, u):
        @pl.when(z == gate_way)
        def _():
            total = row_sums[i, u]
            for m in range(1, span):
                slot = lax.rem(local + m, span)
                far_copy(i, u, near(m), slot).wait_recv()
                total += far_in[i, slot, u].astype(f32)
            cross_out[i, u] = total.astype(bf16)
            push(
                cross_out.at[i, u],
                cross_in.at[i],
                cross_send,
                cross_recv.at[i],
                (at(units[u], x), tp),
            )

    def finish(i):
        total = row_sums[i, own_unit]
        for m in range(1, span):
            near_copies[i, m].wait_recv()
            total += near_in[i, m - 1].astype(f32)
        bulk(cross_in.at[i], cross_send, cross_recv.at[i]).wait_recv()
        total += cross_in[i].astype(f32)
        finished[:, i * LANES : (i + 1) * LANES] = total.astype(bf16)

    far_units, all_units = range(span), range(nz)

    def each(stage, i, which):
        if 0 <= i < chunks:
            for u in which:
                stage(i, u)

    last = chunks - 1
    near_units = range(span, nz)
    for step in range(chunks):
        if step == last:
            each(combine, step - 1, far_units)
        project(step)
        each(combine, step - 1, all_units if step < last else near_units)
        each(spread, step - 2, far_units)
        if step == last:
            for i in range(last - 2):
                each(cross, i, far_units)
        each(spread, step - 2, near_units)
    each(spread, last - 1, far_units)
    each(cross, last - 2, far_units)
    for u in all_units:
        if u > span:
            spread(last, u - span - 1)
        combine(last, u)
        if 0 < u <= span:
            each(cross, last - 1, [u - 1])
        if u < span:
            each(spread, last - 1, [u + span])
    for u in range(span - 1, nz):
        spread(last, u)
        if u - span + 1 < span:
            cross(last, u - span + 1)
    for i in range(chunks):
        finish(i)

    column_to = lax.broadcasted_iota(jnp.int32, (part, part), 1)
    share_to = column_to // source_rows
    inner_to = lax.rem(column_to, source_rows)
    from_to = (inner_to // piece) * LANES + share_to * piece + lax.rem(inner_to, piece)
    order = (lax.broadcasted_iota(jnp.int32, (part, part), 0) == from_to).astype(bf16)
    out[...] = jnp.dot(finished[...], order, preferred_element_type=f32).astype(bf16)

    @pl.when(z == gate_way)
    def _():
        for i in range(span):
            relayed = gathered.at[pl.ds(0, len(beside_half))]
            bulk(relayed, relay_send.at[i], meta_recv).wait_send()
        bulk(cross_out, cross_send, meta_recv).wait_send()

    @pl.when(z != gate_way)
    def _():
        bulk(far_out, far_send, meta_recv).wait_send()

    bulk(meta.at[pl.ds(0, n - 1)], meta_send, meta_recv).wait_send()
    bulk(gathered.at[pl.ds(0, len(beside_half) + 1)], token_send, meta_recv).wait_send()
    bulk(staged, weight_send, meta_recv).wait_send()
    bulk(given, pair_send, meta_recv).wait_send()
    bulk(chip_sums, chip_send, meta_recv).wait_send()
    bulk(x_out, x_send, meta_recv).wait_send()
    bulk(near_out, near_send, meta_recv).wait_send()
    for h in range(1, chips):
        bulk(routed.at[tp], forward_send.at[h], meta_recv).wait_send()
    for copy in shared:
        copy.wait_send()


def settle_kernel(*refs):
    count = (len(refs) - 1) // 2
    sems = refs[-1]
    copies = [
        pltpu.make_async_copy(refs[i], refs[count + i], sems.at[i]) for i in range(count)
    ]
    for copy in copies:
        copy.start()
    for copy in copies:
        copy.wait()


def settle(*arrays):
    anywhere = pl.BlockSpec(memory_space=pl.ANY)
    hbm = pl.BlockSpec(memory_space=pltpu.HBM)
    return pl.pallas_call(
        settle_kernel,
        out_shape=tuple(jax.ShapeDtypeStruct(a.shape, a.dtype) for a in arrays),
        in_specs=[anywhere] * len(arrays),
        out_specs=(hbm,) * len(arrays),
        scratch_shapes=[pltpu.SemaphoreType.DMA((len(arrays),))],
        compiler_params=pltpu.CompilerParams(vmem_limit_bytes=1024 * 1024),
    )(*arrays)


def hand_over(tokens, gain, routes, route_weights, gate_local, up_local, down_local):
    n = lax.axis_size("fs")
    groups = lax.axis_size("tp")
    tok_rows, width = tokens.shape
    top_count = routes.shape[0]
    source_rows, units = gate_local.shape[1:]
    capacity = 3 * tok_rows * top_count // (2 * n)
    total_slots = n * capacity
    part = width // groups
    chips = groups // CORES
    nx = line_width(n)
    nz = n // nx
    span = nz // 2
    chunks = part // LANES
    vmem = pl.BlockSpec(memory_space=pltpu.VMEM)
    hbm = pl.BlockSpec(memory_space=pltpu.HBM)
    bf16, f32 = jnp.bfloat16, jnp.float32
    ready = jax.ShapeDtypeStruct((width, units), bf16)
    dma = pltpu.SemaphoreType.DMA
    rows = (tok_rows, LANES)
    return pl.pallas_call(
        functools.partial(kernel, n, groups, nx, total_slots // 4),
        out_shape=(ready, ready, ready, jax.ShapeDtypeStruct((tok_rows, part), bf16)),
        in_specs=[hbm] * 7,
        out_specs=(vmem,) * 4,
        scratch_shapes=[
            pltpu.VMEM((DEPTH, source_rows, units), f32),
            pltpu.VMEM((tok_rows, width), bf16),
            pltpu.VMEM((1, source_rows), f32),
            pltpu.VMEM((source_rows, 1), f32),
            pltpu.VMEM((tok_rows, 1), f32),
            pltpu.VMEM((top_count, tok_rows), jnp.int32),
            pltpu.VMEM((top_count, tok_rows), bf16),
            pltpu.VMEM((3, n - 1, source_rows, units), bf16),
            pltpu.VMEM((n, tok_rows, part), bf16),
            pltpu.VMEM((n, 8, LANES), f32),
            pltpu.VMEM((n, 8, LANES), f32),
            pltpu.VMEM((n, tok_rows, capacity), bf16),
            pltpu.VMEM((groups, total_slots, part), bf16),
            pltpu.VMEM((total_slots, units), f32),
            pltpu.VMEM((total_slots, units), bf16),
            pltpu.VMEM((chunks, chips, total_slots, LANES), bf16),
            pltpu.VMEM((chunks, chips, total_slots, LANES), bf16),
            pltpu.VMEM((chunks, chips, total_slots, LANES), bf16),
            pltpu.VMEM((chunks, chips - 1, total_slots, LANES), bf16),
            pltpu.VMEM((total_slots, LANES), bf16),
            pltpu.VMEM((chunks, nz) + rows, f32),
            pltpu.VMEM((chunks, nx - 1, nz) + rows, bf16),
            pltpu.VMEM((chunks, nx - 1, nz) + rows, bf16),
            pltpu.VMEM((chunks, span - 1) + rows, bf16),
            pltpu.VMEM((chunks, span - 1) + rows, bf16),
            pltpu.VMEM((chunks, span) + rows, bf16),
            pltpu.VMEM((chunks, span, span) + rows, bf16),
            pltpu.VMEM((chunks, span) + rows, bf16),
            pltpu.VMEM((chunks,) + rows, bf16),
            pltpu.VMEM((tok_rows, part), bf16),
            dma((DEPTH,)),
            dma((5,)),
            dma,
            dma,
            dma,
            dma((span,)),
            dma((n,)),
            dma((chips,)),
            dma((chips,)),
            dma((chips,)),
            dma((chips,)),
            dma,
            dma((2,)),
            dma((chunks,)),
            dma,
            dma((chunks, nz)),
            dma,
            dma((chunks, chips - 1, nz)),
            dma,
            dma((chunks, nx - 1, nz)),
            dma,
            dma((chunks, span - 1)),
            dma,
            dma((chunks, span, span)),
            dma,
            dma((chunks,)),
        ],
        compiler_params=pltpu.CompilerParams(
            collective_id=0, has_side_effects=True, vmem_limit_bytes=44 * 1024 * 1024
        ),
    )(
        *(
            pltpu.with_memory_space_constraint(a, pltpu.HBM)
            for a in (tokens, gain, routes, route_weights, gate_local, up_local, down_local)
        )
    )


def body(tokens, norm_gain, gate_weight, up_weight, down_weight, routes, route_weights):
    gate_ready, up_ready, down_ready, moe_output = hand_over(
        tokens,
        norm_gain[None, :],
        routes.T,
        route_weights.T,
        gate_weight,
        up_weight,
        down_weight,
    )
    return settle(gate_ready[None], up_ready[None], down_ready[None], moe_output)


def solution(mesh):
    in_specs = (
        P("fs", None),
        P("fs"),
        P(None, "fs", "tp"),
        P(None, "fs", "tp"),
        P(None, "fs", "tp"),
        P("fs", None),
        P("fs", None),
    )
    out_specs = (P("fs", None, "tp"), P("fs", None, "tp"), P("fs", None, "tp"), P("fs", "tp"))
    return jax.shard_map(body, mesh=mesh, in_specs=in_specs, out_specs=out_specs, check_vma=False)
```

```python
import functools

import jax
import jax.numpy as jnp
from jax import lax
from jax.experimental import pallas as pl
from jax.experimental.pallas import tpu as pltpu
from jax.sharding import PartitionSpec as P

norm_eps = 1e-06
clamp_limit = 7.0
gate_alpha = 1.702
MESH = pl.DeviceIdType.MESH
CORES = 2
DEPTH = 8
LANES = 128


def activate(gate_pre, up_pre):
    gate_part = jnp.minimum(gate_pre, clamp_limit)
    up_part = jnp.clip(up_pre, -clamp_limit, clamp_limit)
    return (up_part + 1.0) * gate_part * jax.nn.sigmoid(gate_alpha * gate_part)


def line_width(n):
    width = 1
    while 4 * width * width <= n:
        width *= 2
    return width


def kernel(
    n,
    groups,
    nx,
    row_tile,
    tokens,
    gain_in,
    routes_in,
    route_weights_in,
    gate_local,
    up_local,
    down_local,
    gate_ready,
    up_ready,
    down_ready,
    out,
    wide,
    token_rows,
    gain_row,
    gain,
    scale,
    routes,
    route_weights,
    staged,
    gathered,
    meta,
    metas,
    tables,
    routed,
    gate_pre,
    hidden,
    given,
    kept,
    partner_sums,
    chip_sums,
    expert_out,
    row_sums,
    x_out,
    x_in,
    near_out,
    near_in,
    far_out,
    far_in,
    cross_out,
    cross_in,
    finished,
    wide_sem,
    input_sem,
    meta_send,
    meta_recv,
    token_send,
    relay_send,
    token_recv,
    share_send,
    share_recv,
    forward_send,
    forward_recv,
    weight_send,
    weight_recv,
    down_recv,
    pair_send,
    pair_recv,
    chip_send,
    chip_recv,
    x_send,
    x_recv,
    near_send,
    near_recv,
    far_send,
    far_recv,
    cross_send,
    cross_recv,
):
    me = lax.axis_index("fs")
    tp = lax.axis_index("tp")
    chips = groups // CORES
    chip = tp // CORES
    core = lax.rem(tp, CORES)
    partner = chip * CORES + (CORES - 1 - core)
    nz = n // nx
    span = nz // 2
    z = me // nx
    x = lax.rem(me, nx)
    half = z // span
    local = lax.rem(z, span)
    gate_way = span - 1 + half
    far_way = span - half
    tok_rows, width = token_rows.shape
    part = width // groups
    source_rows = gate_local.shape[1]
    shares = n // groups
    total_slots = hidden.shape[0]
    capacity = total_slots // n
    chunks = given.shape[0]
    piece = source_rows // chunks
    f32, bf16 = jnp.float32, jnp.bfloat16

    def at(zz, xx):
        return zz * nx + xx

    def near(i):
        return half * span + lax.rem(local + i, span)

    def far(i):
        return (1 - half) * span + lax.rem(local + i, span)

    def beside(dx):
        return lax.rem(x + dx, nx)

    def slots_of(block):
        return pl.ds(pl.multiple_of(block * capacity, 16), capacity)

    def rows_of(block):
        return pl.ds(pl.multiple_of(block * source_rows, 16), source_rows)

    def chunk_of(block, i):
        return pl.ds(pl.multiple_of(block * source_rows + i * piece, 16), piece)

    group_rows = nx * capacity
    lane_rows = tok_rows // LANES

    def remote(src, dst, send_sem, recv_sem, device):
        return pltpu.make_async_remote_copy(
            src_ref=src,
            dst_ref=dst,
            send_sem=send_sem,
            recv_sem=recv_sem,
            device_id=device,
            device_id_type=MESH,
        )

    def push(src, dst, send_sem, recv_sem, device):
        copy = remote(src, dst, send_sem, recv_sem, device)
        copy.start()
        return copy

    def bulk(ref, send_sem, recv_sem):
        return remote(ref, ref, send_sem, recv_sem, (me, partner))

    peers = [at(far(i), beside(dx)) for dx in range(nx) for i in range(span)]
    peers += [at(near(i), beside(dx)) for dx in range(nx) for i in range(span) if i + dx > 0]
    places = peers + [me]
    locals_ = (gate_local, up_local, down_local)
    readies = (gate_ready, up_ready, down_ready)
    blocks = [(j, q) for j in range(3) for q in range(n)]

    def fetch(i):
        j, q = blocks[i]
        copy = pltpu.make_async_copy(
            locals_[j].at[places[q]], wide.at[i % DEPTH], wide_sem.at[i % DEPTH]
        )
        copy.start()
        return copy

    inputs = [
        pltpu.make_async_copy(src, dst, input_sem.at[spot])
        for spot, (src, dst) in enumerate(
            (
                (gain_in, gain_row),
                (tokens, token_rows),
                (routes_in, routes),
                (route_weights_in, route_weights),
            )
        )
    ]
    own_columns = pl.ds(pl.multiple_of(tp * part, LANES), part)
    inputs.append(
        pltpu.make_async_copy(tokens.at[:, own_columns], gathered.at[me], input_sem.at[4])
    )
    for copy in inputs:
        copy.start()
    fetches = [fetch(i) for i in range(DEPTH)]

    barrier = pltpu.get_barrier_semaphore()
    for k in range(1, n):
        pl.semaphore_signal(
            barrier, inc=1, device_id=(lax.rem(me + k, n), tp), device_id_type=MESH
        )
    for k in range(1, groups):
        pl.semaphore_signal(
            barrier, inc=1, device_id=(me, lax.rem(tp + k, groups)), device_id_type=MESH
        )

    inputs[0].wait()
    gain_at = lax.broadcasted_iota(jnp.int32, (source_rows, source_rows), 0) == (
        lax.broadcasted_iota(jnp.int32, (source_rows, source_rows), 1)
    )
    gain[...] = jnp.sum(jnp.where(gain_at, gain_row[...], 0.0), axis=1, keepdims=True)

    def push_weights(j, q):
        push(
            staged.at[j, q],
            readies[j].at[rows_of(me)],
            weight_send,
            weight_recv.at[j],
            (places[q], tp),
        )

    def convert(i):
        j, q = blocks[i]
        fetches[i].wait()
        value = wide[i % DEPTH]
        if j < 2:
            value = gain[...] * value
        if q == n - 1:
            readies[j][rows_of(me), :] = value.astype(bf16)
        else:
            staged[j, q] = value.astype(bf16)
        if i + DEPTH < len(blocks):
            fetches.append(fetch(i + DEPTH))

    pl.semaphore_wait(barrier, n + groups - 2)

    def push_tokens(block, device_z, device_x):
        push(
            tokens.at[:, own_columns],
            gathered.at[block],
            token_send,
            token_recv.at[block],
            (at(device_z, device_x), tp),
        )

    beside_half = [(i, dx) for dx in range(nx) for i in range(span) if i + dx > 0]
    push_tokens(me, far_way, x)
    for i, dx in beside_half:
        push_tokens(me, near(i), beside(dx))
    convert(0)
    for copy in inputs[1:]:
        copy.wait()

    @pl.loop(0, tok_rows // 32)
    def _(tile):
        rows = pl.ds(pl.multiple_of(tile * 32, 32), 32)
        wide_rows = token_rows[rows, :].astype(f32)
        scale[rows, :] = lax.rsqrt(
            jnp.mean(wide_rows * wide_rows, axis=1, keepdims=True) + norm_eps
        )

    ids = lax.broadcasted_iota(jnp.int32, (n, tok_rows), 0)
    member = jnp.zeros((n, tok_rows), f32)
    row_weight = jnp.zeros((n, tok_rows), f32)
    given_weights = route_weights[...].astype(f32)
    for k in range(routes.shape[0]):
        hit = routes[k : k + 1, :] == ids
        member += jnp.where(hit, 1.0, 0.0)
        row_weight += jnp.where(hit, given_weights[k : k + 1, :], 0.0)
    down_index = lax.broadcasted_iota(jnp.int32, (tok_rows, tok_rows), 0)
    across_index = lax.broadcasted_iota(jnp.int32, (tok_rows, tok_rows), 1)
    before = down_index < across_index
    diagonal = down_index == across_index
    scale_row = jnp.sum(jnp.where(diagonal, scale[...], 0.0), axis=0, keepdims=True)
    counts = jnp.dot(member.astype(bf16), before.astype(bf16), preferred_element_type=f32)
    position = jnp.where(member > 0.0, counts, -1.0)
    meta[...] = jnp.zeros(meta.shape, f32)
    for e in range(n):
        for r in range(lane_rows):
            lanes = slice(r * LANES, (r + 1) * LANES)
            meta[e, r : r + 1, :] = position[e : e + 1, lanes]
            meta[e, lane_rows + r : lane_rows + r + 1, :] = row_weight[e : e + 1, lanes]
            meta[e, 2 * lane_rows + r : 2 * lane_rows + r + 1, :] = scale_row[:, lanes]
    metas[me] = meta[me]

    for k in range(1, n):
        peer = lax.rem(me + k, n)
        push(meta.at[peer], metas.at[me], meta_send, meta_recv, (peer, tp))

    for q in range(1, n):
        convert(q)
        if q <= span:
            push_weights(0, q - 1)
    for q in range(n):
        convert(n + q)

    def push_rest():
        for q in range(span, n - 1):
            push_weights(0, q)

    def push_up():
        for q in range(n - 1):
            push_weights(1, q)

    @pl.when(z != gate_way)
    def _():
        push_rest()
        push_up()

    bulk(metas.at[pl.ds(0, n - 1)], meta_send, meta_recv).wait_recv()

    def await_tokens(block):
        bulk(gathered.at[block], token_send, token_recv.at[block]).wait_recv()

    def share_block(block):
        def to(step, device):
            remote(
                routed.at[tp, slots_of(block)],
                routed.at[tp, slots_of(block)],
                share_send.at[step],
                share_recv.at[step],
                (me, device),
            ).start()

        for h in range(1, chips):
            to(h, lax.rem(chip + h, chips) * CORES + core)
        to(0, partner)

    lines = lax.broadcasted_iota(jnp.int32, (capacity, tok_rows), 0).astype(f32)
    columns_of = lax.broadcasted_iota(jnp.int32, (tok_rows, capacity), 1).astype(f32)
    pending = []

    def pick(block):
        found = metas[block]
        place, weight, scale_across = (
            jnp.concatenate([found[j + r : j + r + 1, :] for r in range(lane_rows)], axis=1)
            for j in (0, lane_rows, 2 * lane_rows)
        )
        chosen = jnp.where(place == lines, 1.0, 0.0).astype(bf16)
        scale_down = jnp.sum(jnp.where(diagonal, scale_across, 0.0), axis=1, keepdims=True)
        normed = (gathered[block].astype(f32) * scale_down).astype(bf16)
        routed[tp, slots_of(block), :] = jnp.dot(
            chosen, normed, preferred_element_type=f32
        ).astype(bf16)
        if pending:
            share_block(pending.pop())
        ones = jnp.ones((tok_rows, capacity), bf16)
        place_down = jnp.dot(
            jnp.where(diagonal, place, 0.0).astype(bf16), ones, preferred_element_type=f32
        )
        weight_down = jnp.dot(
            jnp.where(diagonal, weight, 0.0).astype(bf16), ones, preferred_element_type=f32
        )
        tables[block] = jnp.where(place_down == columns_of, weight_down, 0.0).astype(bf16)
        pending.append(block)

    pick(me)
    for i, dx in beside_half:
        block = at(near(i), beside(dx))
        await_tokens(block)
        pick(block)
    for i in range(span):
        block = at(far(i), x)
        await_tokens(block)

        @pl.when(z == gate_way)
        def _(i=i, block=block):
            for m, dx in beside_half:
                push(
                    gathered.at[block],
                    gathered.at[block],
                    relay_send.at[i],
                    token_recv.at[block],
                    (at(near(m), beside(dx)), tp),
                )

    pl.when(z == gate_way)(push_rest)
    for dx in range(nx):
        for i in range(span):
            block = at(far(i), beside(dx))
            if dx > 0:
                await_tokens(block)
            pick(block)
    share_block(pending.pop())

    pl.when(z == gate_way)(push_up)
    for q in range(n):
        convert(2 * n + q)

    def all_rows(step, origin, device):
        return remote(
            routed.at[tp], routed.at[origin], share_send.at[step], share_recv.at[step], (me, device)
        )

    shared = []
    for h in range(1, chips):
        origin = lax.rem(chip - h + chips, chips) * CORES + core
        copy = all_rows(h, origin, partner)
        copy.wait_recv()
        shared.append(copy)
        push(
            routed.at[origin],
            routed.at[origin],
            forward_send.at[h],
            forward_recv.at[h],
            (me, partner),
        )
    copy = all_rows(0, partner, partner)
    copy.wait_recv()
    shared.append(copy)
    for h in range(1, chips):
        origin = lax.rem(chip - h + chips, chips) * CORES + (CORES - 1 - core)
        remote(
            routed.at[origin],
            routed.at[origin],
            forward_send.at[h],
            forward_recv.at[h],
            (me, partner),
        ).wait_recv()

    def await_weights(j):
        received = readies[j].at[pl.ds(0, (n - 1) * source_rows)]
        bulk(received, weight_send, weight_recv.at[j]).wait_recv()

    def product(rows, ready):
        total = jnp.zeros((row_tile, hidden.shape[1]), f32)
        for t in range(groups):
            total += jnp.dot(
                routed[t, rows, :],
                ready[t * part : (t + 1) * part],
                preferred_element_type=f32,
            )
        return total

    def tiles(body):
        @pl.loop(0, total_slots // row_tile)
        def _(tile):
            body(pl.ds(pl.multiple_of(tile * row_tile, 16), row_tile))

    await_weights(0)

    @tiles
    def _(rows):
        gate_pre[rows, :] = product(rows, gate_ready)

    def push_down(i):
        for q in range(n - 1):
            push(
                staged.at[2, q, pl.ds(i * piece, piece)],
                down_ready.at[chunk_of(me, i)],
                weight_send,
                down_recv.at[i],
                (places[q], tp),
            )

    @pl.when(z == gate_way)
    def _():
        for i in range(chunks):
            push_down(i)

    await_weights(1)
    pl.when(z != gate_way)(functools.partial(push_down, 0))

    @tiles
    def _(rows):
        hidden[rows, :] = activate(gate_pre[rows, :], product(rows, up_ready)).astype(bf16)

    over_copies = {}
    units = [(1 - half) * span + f for f in range(span)]
    units += [near(m) for m in range(1, span)] + [z]
    mates = range(span, nz - 1)
    own_unit = nz - 1

    def rows_in(u):
        return pl.ds(pl.multiple_of(units[u] * group_rows, 16), group_rows)

    def project(i):
        received = down_ready.at[pl.ds(0, (n - 1) * piece)]
        bulk(received, weight_send, down_recv.at[i]).wait_recv()
        if i + 1 < chunks:
            pl.when(z != gate_way)(functools.partial(push_down, i + 1))

        def rows_to(side):
            picked = [
                down_ready[
                    chunk_of((lax.rem(chip + h, chips) * CORES + side) * shares + r, i), :
                ]
                for h in range(chips)
                for r in range(shares)
            ]
            return jnp.concatenate(picked, axis=0)

        def run(down, target, u):
            rows = rows_in(u)
            value = lax.dot_general(
                hidden[rows, :], down, (((1,), (1,)), ((), ())), preferred_element_type=f32
            ).astype(bf16)
            for h in range(chips):
                target[i, h, rows, :] = value[:, h * LANES : (h + 1) * LANES]

        give = rows_to(CORES - 1 - core)
        for u in range(nz):
            run(give, given, u)
            for h in range(chips):
                push(
                    given.at[i, h, rows_in(u)],
                    partner_sums.at[i, h, rows_in(u)],
                    pair_send,
                    pair_recv.at[i, u],
                    (me, partner),
                )
        keep = rows_to(core)
        for u in range(nz):
            rows = rows_in(u)
            run(keep, kept, u)
            bulk(given.at[i, pl.ds(0, chips), rows], pair_send, pair_recv.at[i, u]).wait_recv()
            for h in range(1, chips):
                total = kept[i, h, rows, :].astype(f32)
                total += partner_sums[i, h, rows, :].astype(f32)
                kept[i, h, rows, :] = total.astype(bf16)
                over_copies[i, h, u] = push(
                    kept.at[i, h, rows],
                    chip_sums.at[i, h - 1, rows],
                    chip_send,
                    chip_recv.at[i, h - 1, u],
                    (me, lax.rem(chip + h, chips) * CORES + core),
                )

    x_copies = {}

    def combine(i, u):
        for h in range(1, chips):
            over_copies[i, h, u].wait_recv()

        rows = rows_in(u)
        total = kept[i, 0, rows, :].astype(f32) + partner_sums[i, 0, rows, :].astype(f32)
        for h in range(1, chips):
            total += chip_sums[i, h - 1, rows, :].astype(f32)
        expert_out[rows, :] = total.astype(bf16)

        def rows_for(xx):
            block = at(units[u], xx)
            return jnp.dot(
                tables[block], expert_out[slots_of(block), :], preferred_element_type=f32
            )

        for dx in range(1, nx):
            x_out[i, dx - 1, u] = rows_for(beside(dx)).astype(bf16)
            x_copies[i, dx, u] = push(
                x_out.at[i, dx - 1, u],
                x_in.at[i, dx - 1, u],
                x_send,
                x_recv.at[i, dx - 1, u],
                (at(z, beside(dx)), tp),
            )
        row_sums[i, u] = rows_for(x)

    near_copies = {}

    def far_copy(i, u, device_z, slot):
        return remote(
            far_out.at[i, u],
            far_in.at[i, slot, u],
            far_send,
            far_recv.at[i, slot, u],
            (at(device_z, x), tp),
        )

    def spread(i, u):
        for dx in range(1, nx):
            x_copies[i, dx, u].wait_recv()
        total = row_sums[i, u]
        for dx in range(1, nx):
            total += x_in[i, dx - 1, u].astype(f32)
        row_sums[i, u] = total
        if u < span:

            @pl.when(z != gate_way)
            def _():
                far_out[i, u] = total.astype(bf16)
                far_copy(i, u, gate_way, local).start()

        elif u in mates:
            m = u - span + 1
            near_out[i, m - 1] = total.astype(bf16)
            near_copies[i, m] = push(
                near_out.at[i, m - 1],
                near_in.at[i, m - 1],
                near_send,
                near_recv.at[i, m - 1],
                (at(near(m), x), tp),
            )

    def cross(i, u):
        @pl.when(z == gate_way)
        def _():
            total = row_sums[i, u]
            for m in range(1, span):
                slot = lax.rem(local + m, span)
                far_copy(i, u, near(m), slot).wait_recv()
                total += far_in[i, slot, u].astype(f32)
            cross_out[i, u] = total.astype(bf16)
            push(
                cross_out.at[i, u],
                cross_in.at[i],
                cross_send,
                cross_recv.at[i],
                (at(units[u], x), tp),
            )

    def finish(i):
        total = row_sums[i, own_unit]
        for m in range(1, span):
            near_copies[i, m].wait_recv()
            total += near_in[i, m - 1].astype(f32)
        bulk(cross_in.at[i], cross_send, cross_recv.at[i]).wait_recv()
        total += cross_in[i].astype(f32)
        finished[:, i * LANES : (i + 1) * LANES] = total.astype(bf16)

    far_units, all_units = range(span), range(nz)

    def each(stage, i, which):
        if 0 <= i < chunks:
            for u in which:
                stage(i, u)

    last = chunks - 1
    near_units = range(span, nz)
    for step in range(chunks):
        if step == last:
            each(combine, step - 1, far_units)
        project(step)
        each(combine, step - 1, all_units if step < last else near_units)
        each(spread, step - 2, far_units)
        if step == last:
            for i in range(last - 2):
                each(cross, i, far_units)
        each(spread, step - 2, near_units)
    each(spread, last - 1, far_units)
    each(cross, last - 2, far_units)
    for u in all_units:
        if u > span:
            spread(last, u - span - 1)
        combine(last, u)
        if 0 < u <= span:
            each(cross, last - 1, [u - 1])
        if u < span:
            each(spread, last - 1, [u + span])
    for u in range(span - 1, nz):
        spread(last, u)
        if u - span + 1 < span:
            cross(last, u - span + 1)
    for i in range(chunks):
        finish(i)

    column_to = lax.broadcasted_iota(jnp.int32, (part, part), 1)
    share_to = column_to // source_rows
    inner_to = lax.rem(column_to, source_rows)
    from_to = (inner_to // piece) * LANES + share_to * piece + lax.rem(inner_to, piece)
    order = (lax.broadcasted_iota(jnp.int32, (part, part), 0) == from_to).astype(bf16)
    out[...] = jnp.dot(finished[...], order, preferred_element_type=f32).astype(bf16)

    @pl.when(z == gate_way)
    def _():
        for i in range(span):
            relayed = gathered.at[pl.ds(0, len(beside_half))]
            bulk(relayed, relay_send.at[i], meta_recv).wait_send()
        bulk(cross_out, cross_send, meta_recv).wait_send()

    @pl.when(z != gate_way)
    def _():
        bulk(far_out, far_send, meta_recv).wait_send()

    bulk(meta.at[pl.ds(0, n - 1)], meta_send, meta_recv).wait_send()
    bulk(gathered.at[pl.ds(0, len(beside_half) + 1)], token_send, meta_recv).wait_send()
    bulk(staged, weight_send, meta_recv).wait_send()
    bulk(given, pair_send, meta_recv).wait_send()
    bulk(chip_sums, chip_send, meta_recv).wait_send()
    bulk(x_out, x_send, meta_recv).wait_send()
    bulk(near_out, near_send, meta_recv).wait_send()
    for h in range(1, chips):
        bulk(routed.at[tp], forward_send.at[h], meta_recv).wait_send()
    for copy in shared:
        copy.wait_send()


def settle_kernel(*refs):
    count = (len(refs) - 1) // 2
    sems = refs[-1]
    copies = [
        pltpu.make_async_copy(refs[i], refs[count + i], sems.at[i]) for i in range(count)
    ]
    for copy in copies:
        copy.start()
    for copy in copies:
        copy.wait()


def settle(*arrays):
    anywhere = pl.BlockSpec(memory_space=pl.ANY)
    hbm = pl.BlockSpec(memory_space=pltpu.HBM)
    return pl.pallas_call(
        settle_kernel,
        out_shape=tuple(jax.ShapeDtypeStruct(a.shape, a.dtype) for a in arrays),
        in_specs=[anywhere] * len(arrays),
        out_specs=(hbm,) * len(arrays),
        scratch_shapes=[pltpu.SemaphoreType.DMA((len(arrays),))],
        compiler_params=pltpu.CompilerParams(vmem_limit_bytes=1024 * 1024),
    )(*arrays)


def hand_over(tokens, gain, routes, route_weights, gate_local, up_local, down_local):
    n = lax.axis_size("fs")
    groups = lax.axis_size("tp")
    tok_rows, width = tokens.shape
    top_count = routes.shape[0]
    source_rows, units = gate_local.shape[1:]
    capacity = 3 * tok_rows * top_count // (2 * n)
    total_slots = n * capacity
    part = width // groups
    chips = groups // CORES
    nx = line_width(n)
    nz = n // nx
    span = nz // 2
    chunks = part // LANES
    vmem = pl.BlockSpec(memory_space=pltpu.VMEM)
    hbm = pl.BlockSpec(memory_space=pltpu.HBM)
    bf16, f32 = jnp.bfloat16, jnp.float32
    ready = jax.ShapeDtypeStruct((width, units), bf16)
    dma = pltpu.SemaphoreType.DMA
    rows = (tok_rows, LANES)
    return pl.pallas_call(
        functools.partial(kernel, n, groups, nx, total_slots // 4),
        out_shape=(ready, ready, ready, jax.ShapeDtypeStruct((tok_rows, part), bf16)),
        in_specs=[hbm] * 7,
        out_specs=(vmem,) * 4,
        scratch_shapes=[
            pltpu.VMEM((DEPTH, source_rows, units), f32),
            pltpu.VMEM((tok_rows, width), bf16),
            pltpu.VMEM((1, source_rows), f32),
            pltpu.VMEM((source_rows, 1), f32),
            pltpu.VMEM((tok_rows, 1), f32),
            pltpu.VMEM((top_count, tok_rows), jnp.int32),
            pltpu.VMEM((top_count, tok_rows), bf16),
            pltpu.VMEM((3, n - 1, source_rows, units), bf16),
            pltpu.VMEM((n, tok_rows, part), bf16),
            pltpu.VMEM((n, 8, LANES), f32),
            pltpu.VMEM((n, 8, LANES), f32),
            pltpu.VMEM((n, tok_rows, capacity), bf16),
            pltpu.VMEM((groups, total_slots, part), bf16),
            pltpu.VMEM((total_slots, units), f32),
            pltpu.VMEM((total_slots, units), bf16),
            pltpu.VMEM((chunks, chips, total_slots, LANES), bf16),
            pltpu.VMEM((chunks, chips, total_slots, LANES), bf16),
            pltpu.VMEM((chunks, chips, total_slots, LANES), bf16),
            pltpu.VMEM((chunks, chips - 1, total_slots, LANES), bf16),
            pltpu.VMEM((total_slots, LANES), bf16),
            pltpu.VMEM((chunks, nz) + rows, f32),
            pltpu.VMEM((chunks, nx - 1, nz) + rows, bf16),
            pltpu.VMEM((chunks, nx - 1, nz) + rows, bf16),
            pltpu.VMEM((chunks, span - 1) + rows, bf16),
            pltpu.VMEM((chunks, span - 1) + rows, bf16),
            pltpu.VMEM((chunks, span) + rows, bf16),
            pltpu.VMEM((chunks, span, span) + rows, bf16),
            pltpu.VMEM((chunks, span) + rows, bf16),
            pltpu.VMEM((chunks,) + rows, bf16),
            pltpu.VMEM((tok_rows, part), bf16),
            dma((DEPTH,)),
            dma((5,)),
            dma,
            dma,
            dma,
            dma((span,)),
            dma((n,)),
            dma((chips,)),
            dma((chips,)),
            dma((chips,)),
            dma((chips,)),
            dma,
            dma((2,)),
            dma((chunks,)),
            dma,
            dma((chunks, nz)),
            dma,
            dma((chunks, chips - 1, nz)),
            dma,
            dma((chunks, nx - 1, nz)),
            dma,
            dma((chunks, span - 1)),
            dma,
            dma((chunks, span, span)),
            dma,
            dma((chunks,)),
        ],
        compiler_params=pltpu.CompilerParams(
            collective_id=0, has_side_effects=True, vmem_limit_bytes=44 * 1024 * 1024
        ),
    )(
        *(
            pltpu.with_memory_space_constraint(a, pltpu.HBM)
            for a in (tokens, gain, routes, route_weights, gate_local, up_local, down_local)
        )
    )


def body(tokens, norm_gain, gate_weight, up_weight, down_weight, routes, route_weights):
    gate_ready, up_ready, down_ready, moe_output = hand_over(
        tokens,
        norm_gain[None, :],
        routes.T,
        route_weights.T,
        gate_weight,
        up_weight,
        down_weight,
    )
    return settle(gate_ready[None], up_ready[None], down_ready[None], moe_output)


def solution(mesh):
    in_specs = (
        P("fs", None),
        P("fs"),
        P(None, "fs", "tp"),
        P(None, "fs", "tp"),
        P(None, "fs", "tp"),
        P("fs", None),
        P("fs", None),
    )
    out_specs = (P("fs", None, "tp"), P("fs", None, "tp"), P("fs", None, "tp"), P("fs", "tp"))
    return jax.shard_map(body, mesh=mesh, in_specs=in_specs, out_specs=out_specs, check_vma=False)
```
